512 devices in a mesh: sp: 32 (over z, x), tp: 16 (over y, core).
Axes of the slice: x: 4, y: 8, z: 8, core: 2. Of those that a mesh axis runs over, the one named last changes fastest.
Arguments:
- pool_input: bfloat16 [4096, 1024], P('sp', 'tp'), may hold values from -12 to 12
- doc_ids: int32 [4096], P('sp'), may hold values from 0 to 7, as said below
- residual: bfloat16 [4096, 2048], P('sp', 'tp'), may hold values from -30 to 30
- pool_gain: float32 [1024], P('tp'), may hold values from 0.1 to 1.9
- out_proj: bfloat16 [1024, 2048], P('tp'), may hold values from -0.25 to 0.25
- norm_gain: float32 [2048], P('tp'), may hold values from 0.1 to 1.9
- routes: int32 [4096, 2], P('sp'), may hold values from 0 to 31, all different within a row; in each aligned block of 128 rows (0 to 127, 128 to 255, ...) at most 16 rows name the same one
- route_weights: float32 [4096, 2], P('sp'), may hold values from 0.2 to 1.2
- expert_gate: bfloat16 [32, 2048, 4096], P('sp', None, 'tp'), may hold values from -0.125 to 0.125
- expert_up: bfloat16 [32, 2048, 4096], P('sp', None, 'tp'), may hold values from -0.125 to 0.125
- expert_down: bfloat16 [32, 4096, 2048], P('sp', 'tp'), may hold values from -0.125 to 0.125
- shared_gate: bfloat16 [2048, 1024], P(None, 'tp'), may hold values from -0.125 to 0.125
- shared_up: bfloat16 [2048, 1024], P(None, 'tp'), may hold values from -0.125 to 0.125
- shared_down: bfloat16 [1024, 2048], P('tp'), may hold values from -0.25 to 0.25
Outputs:
- layer_out: bfloat16 [4096, 2048], P('sp', 'tp')
The draws below stay inside these ranges and needn't reach their ends.
Inputs may be any that keep to these rules, and one draw needn't show every extreme that they name: `routes`: each row names 2 different experts. In each aligned block of 128 rows no expert is named by more than 16 rows; in some blocks one expert is named by exactly 16 rows. `doc_ids`: document numbers start at 0, never fall along the sequence and rise by one at each document's start.
All inputs are finite; a program needn't handle non-finite values.
Results may differ from the reference program's by a relative error of at most 0.015.
Values may be sent and summed in bfloat16 or wider, within the bound.
No kernel may reach another device: no remote copies, remote signals or barrier semaphores. Data moves between devices by JAX's collectives and lax.ppermute only.
A program may use at most 64 MiB of HBM per device.

```python
import math
import jax
import jax.numpy as jnp
import numpy as np
from jax import lax

D = 2048
PW = 1024
FF_E = 4096
FF_S = 1024
TOP_K = 2
TOK_DEV = 128
TOKENS = 4096
EXPERTS = 32
CAP = 16
N_SP = 32
N_TP = 16


def draw_doc_ids(key, part):
    documents = max(2, N_SP // 4)
    spacing = TOKENS // documents
    offsets = jax.random.randint(jax.random.fold_in(key, 31), (documents - 1,), TOK_DEV // 4, 3 * TOK_DEV // 4 + 1)
    starts = jnp.arange(1, documents, dtype=jnp.int32) * spacing + offsets.astype(jnp.int32)
    positions = jnp.arange(TOKENS, dtype=jnp.int32)
    return jnp.sum((positions[:, None] >= starts[None, :]).astype(jnp.int32), axis=1).astype(jnp.int32)


def draw_pool_input(key, part):
    noise_key, level_key = jax.random.split(jax.random.fold_in(key, 11))
    levels = jax.random.normal(level_key, (TOKENS // 16, PW), jnp.float32)
    levels = jnp.repeat(levels, 16, axis=0)
    noise = jax.random.normal(noise_key, (TOKENS, PW), jnp.float32)
    values = noise + 1.5 * levels
    return jnp.clip(values, -12.0, 12.0).astype(jnp.bfloat16)


def draw_residual(key, part):
    noise_key, column_key = jax.random.split(jax.random.fold_in(key, 23))
    position = jnp.arange(D, dtype=jnp.float32) / (D - 1)
    noise = jax.random.normal(noise_key, (TOKENS, D), jnp.float32)
    scales = jnp.exp(jnp.log(3.0) * position + jax.random.uniform(column_key, (D,), jnp.float32, -0.5, 0.5))
    return jnp.clip(noise * scales[None, :], -30.0, 30.0).astype(jnp.bfloat16)


def strengthened(array, rng, source, target, shards_of, factor):
    def block_of(dim):
        return (jnp.arange(array.shape[dim]) // (array.shape[dim] // shards_of)).reshape((-1,) + (1,) * (array.ndim - 1 - dim))

    one_side = jax.random.permutation(rng, shards_of)[block_of(target)]
    far = (block_of(target) + shards_of // 2) % shards_of
    return jnp.where((block_of(source) == one_side) | (block_of(source) == far), factor * array, array)


def block_scale(rng, extent, cuts, least, high):
    level = 1.0
    for dim, parts in cuts:
        draws = jax.random.uniform(jax.random.fold_in(jax.random.fold_in(rng, 6), dim), (parts,), jnp.float32, least / len(cuts), high / len(cuts))
        level = level * jnp.repeat(jnp.exp(draws), extent[dim] // parts).reshape((-1,) + (1,) * (len(extent) - 1 - dim))
    return level


def assign_block(rng, own, number, rows, number_of, top, reach, skew):
    ranking = jax.random.permutation(rng, number_of)
    crowded, usual = portions_of(number_of, rows * top, reach, skew, True), portions_of(number_of, rows * top, reach, skew, False)
    places = jnp.arange(number_of)

    def named(lengths, turn):
        used = int((lengths > 0).sum())
        fixed = max(1, used // 4)
        passed = fixed + (places - fixed + turn * (used - fixed)) % max(1, number_of - fixed)
        return jnp.zeros((number_of,), jnp.int32).at[ranking[jnp.where(places < fixed, places, passed)]].set(jnp.asarray(lengths, jnp.int32))

    lengths = jnp.where(number % 4 == 0, named(crowded, number // 4), named(usual, number - number // 4 - 1))
    mixed = jax.random.permutation(jax.random.fold_in(own, 3), number_of)
    source_of, receiver = mixed[0:number_of // 2 * 2:2], mixed[1:number_of // 2 * 2:2]
    room = jnp.minimum(lengths[source_of] - 1, reach - lengths[receiver]) // 2
    room = jnp.where((source_of == ranking[0]) | (receiver == ranking[0]) | (lengths[receiver] == 0), 0, jnp.maximum(room, 0))
    passed = jax.random.randint(jax.random.fold_in(own, 4), (number_of // 2,), 0, 1 << 20) % (room + 1)
    lengths = lengths.at[source_of].add(-passed).at[receiver].add(passed)
    labels = jnp.searchsorted(jnp.cumsum(lengths), jnp.arange(rows * top), side="right").astype(jnp.int32)
    grid = labels.reshape(top, rows).T
    grid = grid[jax.random.permutation(jax.random.fold_in(own, 1), rows)]
    turn = jax.random.randint(jax.random.fold_in(own, 2), (rows, 1), 0, top)
    return jnp.take_along_axis(grid, (jnp.arange(top)[None, :] + turn) % top, axis=1)


def portions_of(count, total, limit, slope, full):
    loads = [(1 << 20) // math.isqrt(rank ** slope) + 1 for rank in range(1, count + 1)]
    largest = limit if full else min(limit, max(-(-total // count), total * loads[0] // sum(loads)))
    least = 1 if total - largest >= count - 1 else 0
    holding, spare = [largest] + [least] * (count - 1), total - largest - least * (count - 1)
    while spare > 0:
        movable = [i for i in range(1, count) if holding[i] < largest] or [i for i in range(1, count) if holding[i] < limit]
        mass, left = sum([loads[i] for i in movable]), spare
        for i in movable:
            extra = min(limit - holding[i], max(1, left * loads[i] // mass), spare)
            holding[i] = holding[i] + extra
            spare = spare - extra
    return np.array(holding)


def centred(key, dims, spread, limit, cuts=(), kind=jnp.bfloat16):
    drawn = jax.random.normal(key, dims, jnp.float32) * spread
    if len(cuts) > 0:
        drawn = block_scale(key, dims, cuts, -0.22, 0.18) * drawn
    return jnp.clip(drawn, min=-limit, max=limit).astype(kind)


def bell_draw_with(key, extent, spread, most, cuts, heavy, kind=jnp.bfloat16):
    values = spread * jax.random.normal(key, extent, jnp.float32)
    if cuts:
        values = values * block_scale(key, extent, cuts, -0.22, 0.18)
    return jnp.clip(strengthened(values, jax.random.fold_in(key, 3), *heavy), -most, most).astype(kind)


def setup_inputs(seed: int = 0) -> dict:
    arg_keys = jax.random.split(jax.random.key(seed), 15)
    pool_input = draw_pool_input(jax.random.fold_in(arg_keys[14], 71), 0)
    doc_ids = draw_doc_ids(jax.random.fold_in(arg_keys[14], 71), 0)
    residual = draw_residual(jax.random.fold_in(arg_keys[14], 71), 0)
    pool_gain = jnp.clip(1.0 + 0.18 * jax.random.normal(arg_keys[3], (PW,), jnp.float32), 0.1, 1.9)
    out_proj = bell_draw_with(arg_keys[4], (PW, D), PW ** -0.5, 0.25, ((0, 16),), (0, 1, 16, 2.0))
    norm_gain = jnp.clip(1.0 + 0.18 * jax.random.normal(arg_keys[5], (D,), jnp.float32), 0.1, 1.9)
    routes_keys = jax.random.split(jax.random.fold_in(arg_keys[6], 1), TOKENS // TOK_DEV)
    routes_turns = jax.random.permutation(jax.random.fold_in(arg_keys[6], 3), TOKENS // TOK_DEV)
    routes = jax.vmap(lambda own, number: assign_block(jax.random.fold_in(arg_keys[6], 2), own, number, TOK_DEV, EXPERTS, TOP_K, CAP, 1))(routes_keys, routes_turns).reshape((TOKENS, TOP_K))
    route_weights = jnp.clip(jnp.exp(math.log(1.2) - 1.7917595 * jax.random.uniform(arg_keys[7], (TOKENS, TOP_K), jnp.float32) ** block_scale(arg_keys[7], (TOKENS, TOP_K), ((0, 32),), -0.2, 0.2)), 0.2, 1.2)
    expert_gate = centred(arg_keys[8], (EXPERTS, D, FF_E), D ** -0.5, 0.125, ((0, 32), (2, 16)))
    expert_up = centred(arg_keys[9], (EXPERTS, D, FF_E), D ** -0.5, 0.125, ((0, 32), (2, 16)))
    expert_down = bell_draw_with(arg_keys[10], (EXPERTS, FF_E, D), FF_E ** -0.5, 0.125, ((0, 32), (1, 16)), (1, 2, 16, 2.0))
    shared_gate = centred(arg_keys[11], (D, FF_S), D ** -0.5, 0.125, ((1, 16),))
    shared_up = centred(arg_keys[12], (D, FF_S), D ** -0.5, 0.125, ((1, 16),))
    shared_down = bell_draw_with(arg_keys[13], (FF_S, D), FF_S ** -0.5, 0.25, ((0, 16),), (0, 1, 16, 2.0))
    return {"pool_input": pool_input, "doc_ids": doc_ids, "residual": residual, "pool_gain": pool_gain, "out_proj": out_proj, "norm_gain": norm_gain, "routes": routes, "route_weights": route_weights, "expert_gate": expert_gate, "expert_up": expert_up, "expert_down": expert_down, "shared_gate": shared_gate, "shared_up": shared_up, "shared_down": shared_down}


def blocked_down(hidden, down_weight, groups):
    width = hidden.shape[1] // groups
    pieces = jnp.moveaxis(hidden.reshape(hidden.shape[0], groups, width), 1, 0)
    weights = down_weight.reshape(groups, width, down_weight.shape[1])

    def add_group(accumulated, pair):
        product = jnp.dot(pair[0], pair[1], preferred_element_type=jnp.float32)
        rounded = lax.optimization_barrier(product.astype(jnp.bfloat16))
        return (accumulated + rounded.astype(jnp.float32), None)
    initial = jnp.zeros((hidden.shape[0], down_weight.shape[1]), jnp.float32)
    summed, unused = lax.scan(add_group, initial, (pieces, weights))
    return summed.astype(jnp.bfloat16)

def reference(pool_input, doc_ids, residual, pool_gain, out_proj, norm_gain, routes, route_weights, expert_gate, expert_up, expert_down, shared_gate, shared_up, shared_down):
    values = pool_input.astype(jnp.float32)
    positions = jnp.arange(TOKENS, dtype=jnp.int32)
    begins = jnp.concatenate([jnp.ones((1,), bool), doc_ids[1:] != doc_ids[:-1]])
    doc_start = lax.cummax(jnp.where(begins, positions, 0), axis=0)
    length = (positions - doc_start + 1).astype(jnp.float32)
    scale_index = jnp.arange(PW, dtype=jnp.int32) % 4
    window_size = jnp.where(scale_index == 0, 2.0, jnp.where(scale_index == 1, 8.0, 16.0))
    padded = jnp.concatenate([jnp.zeros((15, PW), jnp.float32), values], 0)
    window_total = jnp.zeros((TOKENS, PW), jnp.float32)
    for offset in range(16):
        inside = (offset < length[:, None]) & (offset < window_size[None, :])
        window_total = window_total + jnp.where(inside, padded[15 - offset:15 - offset + TOKENS], 0.0)
    window_mean = window_total / jnp.minimum(length[:, None], window_size[None, :])
    running = jnp.cumsum(values[:, 3::4], axis=0)
    shifted = jnp.concatenate([jnp.zeros((1, PW // 4), jnp.float32), running], 0)
    doc_sum = running - jnp.take(shifted, doc_start, axis=0)
    doc_mean = doc_sum / length[:, None]
    pool_mean = jnp.concatenate([window_mean.reshape(TOKENS, PW // 4, 4)[..., :3], doc_mean[..., None]], -1)
    pool_mean = pool_mean.reshape(TOKENS, PW)
    pooled = ((pool_mean - values) * pool_gain).astype(jnp.bfloat16)
    projected = blocked_down(pooled, out_proj, N_TP)
    hidden_state = residual.astype(jnp.float32) + projected.astype(jnp.float32)
    squares = lax.optimization_barrier(jnp.mean(hidden_state * hidden_state, axis=1, keepdims=True))
    normed = (hidden_state * lax.rsqrt(squares + 1e-06) * norm_gain).astype(jnp.bfloat16)
    flat_experts = routes.reshape(N_SP, TOK_DEV * TOP_K)
    onehot = (flat_experts[..., None] == jnp.arange(EXPERTS, dtype=jnp.int32)).astype(jnp.int32)
    ranks = lax.optimization_barrier(jnp.sum((jnp.cumsum(onehot, axis=1) - 1) * onehot, axis=2))
    block_ids = jnp.arange(N_SP, dtype=jnp.int32)[:, None]
    slot_index = ((flat_experts * N_SP + block_ids) * CAP + ranks).reshape(-1).astype(jnp.int32)
    token_index = (jnp.arange(TOKENS * TOP_K, dtype=jnp.int32) // TOP_K).astype(jnp.int32)
    table_rows = EXPERTS * N_SP * CAP
    slot_token = jnp.full((table_rows,), TOKENS, jnp.int32).at[slot_index].set(token_index)
    with_blank = jnp.concatenate([normed, jnp.zeros((1, D), jnp.bfloat16)], 0)
    expert_rows = jnp.take(with_blank, slot_token, axis=0).reshape(EXPERTS, N_SP * CAP, D)

    def run_expert(group):
        rows_in, gate_weight, up_weight, down_weight = group
        gate = jnp.dot(rows_in, gate_weight, preferred_element_type=jnp.float32)
        upper = jnp.dot(rows_in, up_weight, preferred_element_type=jnp.float32)
        hidden = (jax.nn.silu(gate) * upper).astype(jnp.bfloat16)
        return blocked_down(hidden, down_weight, N_TP)
    expert_out = lax.map(run_expert, (expert_rows, expert_gate, expert_up, expert_down)).reshape(table_rows, D)
    picked = jnp.take(expert_out, slot_index, axis=0).astype(jnp.float32) * route_weights.reshape(-1)[:, None]
    routed = lax.optimization_barrier(jnp.sum(picked.reshape(TOKENS, TOP_K, D), axis=1))
    shared_gate_out = jnp.dot(normed, shared_gate, preferred_element_type=jnp.float32)
    shared_up_out = jnp.dot(normed, shared_up, preferred_element_type=jnp.float32)
    shared_hidden = (jax.nn.silu(shared_gate_out) * shared_up_out).astype(jnp.bfloat16)
    shared_out = blocked_down(shared_hidden, shared_down, N_TP)
    return (hidden_state + routed + shared_out.astype(jnp.float32)).astype(jnp.bfloat16)
```

```python
import jax
import jax.numpy as jnp
from jax import lax
from jax.experimental import pallas as pl
from jax.experimental.pallas import tpu as pltpu
from jax.sharding import Mesh
from jax.sharding import PartitionSpec as P

F32 = jnp.float32
BF16 = jnp.bfloat16
SUM_LANE = 64
W_LANE = 80
META_LANE = 88


def exchanged(value, axis):
    return lax.all_to_all(value, axis, split_axis=0, concat_axis=0, tiled=True)


def three_parts(value):
    first = value.astype(BF16).astype(F32)
    second = (value - first).astype(BF16).astype(F32)
    third = (value - first - second).astype(BF16).astype(F32)
    return first, second, third


def iota(shape, dim):
    return lax.broadcasted_iota(jnp.int32, shape, dim)


def matmul(a, b):
    return jnp.dot(a, b, preferred_element_type=F32)


def opening(pool_ref, docs_ref, routes_ref, weights_ref, message_ref, slots_ref):
    rows, channels = pool_ref.shape
    square = (rows, rows)
    across = iota((channels, 128), 0)
    lane = iota((channels, 128), 1)
    spread = (lane == across) | ((across % 4 == 3) & (lane == SUM_LANE + across // 4))
    wide = matmul(pool_ref[...], spread.astype(F32).astype(BF16))
    docs = docs_ref[...].astype(F32)
    last_doc = docs[:, rows - 1 :]
    trailing = (docs == last_doc).astype(F32)
    sums = matmul(jnp.broadcast_to(trailing, (8, rows)).astype(BF16), wide.astype(BF16))[0:1]
    count = jnp.sum(trailing, axis=1, keepdims=True)

    columns = [jnp.broadcast_to(routes_ref[:, k : k + 1].astype(F32), square) for k in (0, 1)]
    lines = [column.T for column in columns]
    before = iota(square, 0) < iota(square, 1)

    def counted(mask):
        return jnp.sum(mask.astype(F32), axis=0, keepdims=True)

    first_rank = counted((columns[0] == lines[0]) & before)
    second_rank = counted(columns[0] == lines[1]) + counted((columns[1] == lines[1]) & before)
    first_slot = lines[0][0:1] * 16.0 + first_rank
    second_slot = lines[1][0:1] * 16.0 + second_rank
    slots_ref[...] = jnp.concatenate(
        [first_slot, second_slot, jnp.zeros((6, rows), F32)], axis=0
    )
    share = [
        jnp.broadcast_to(weights_ref[:, k : k + 1], square).T[0:1] for k in (0, 1)
    ]
    slot = iota((512, rows), 0).astype(F32)
    is_first = slot == first_slot
    is_second = slot == second_slot
    weight = jnp.sum(
        jnp.where(is_first, share[0], 0.0) + jnp.where(is_second, share[1], 0.0),
        axis=1,
        keepdims=True,
    )
    chosen_first = jnp.sum(is_first.astype(F32), axis=1, keepdims=True)

    row = iota((16, 128), 0)
    at = iota((16, 128), 1)
    parts = three_parts(sums)
    shared = jnp.where(at < channels, wide[rows - 16 :], 0.0)
    in_sums = (at >= SUM_LANE) & (at < SUM_LANE + 16)
    for k in range(3):
        shared = jnp.where(in_sums & (row == k), parts[k], shared)
    doc_high = jnp.floor(last_doc * (1.0 / 128.0))
    doc_low = last_doc - doc_high * 128.0
    for k, value in enumerate((count, doc_high, doc_low)):
        shared = jnp.where(at == META_LANE + k, value, shared)
    place = iota((512, 128), 1)
    message = jnp.broadcast_to(shared[None], (32, 16, 128)).reshape(512, 128)
    for k, value in enumerate((*three_parts(weight), chosen_first)):
        message = jnp.where(place == W_LANE + k, value, message)
    message_ref[...] = message.reshape(32, 16, 128).astype(BF16)


def pooling(
    index_ref, arrived_ref, pool_ref, docs_ref, gain_ref, project_ref, norm_ref, out_ref
):
    rows, channels = pool_ref.shape
    own = index_ref[0]
    docs = docs_ref[...].astype(F32)
    first_doc = docs[:, 0:1]
    arrived = arrived_ref[...].astype(F32)
    meta = arrived[:, 0:1]
    their_count = meta[:, :, META_LANE : META_LANE + 1]
    their_doc = (
        meta[:, :, META_LANE + 1 : META_LANE + 2] * 128.0
        + meta[:, :, META_LANE + 2 : META_LANE + 3]
    )
    block = iota((32, 1, 1), 0)
    joins = (block < own) & (their_doc == first_doc.reshape(1, 1, 1))
    carry_length = jnp.sum(jnp.where(joins, their_count, 0.0), axis=0)
    sums = jnp.sum(jnp.where(joins, arrived[:, 0:8], 0.0), axis=0)
    sums = jnp.where(iota((8, 128), 0) < 3, sums, 0.0)
    back = (iota((128, channels), 0) == SUM_LANE + iota((128, channels), 1) // 4) & (
        iota((128, channels), 1) % 4 == 3
    )
    total = jnp.sum(sums, axis=0, keepdims=True)
    carry = sum(
        matmul(jnp.broadcast_to(part, (8, 128)).astype(BF16), back.astype(F32).astype(BF16))
        for part in three_parts(total)
    )[0:1]

    behind = block == own - 1
    rim = jnp.sum(jnp.where(behind, arrived, 0.0), axis=0)[:, :channels]
    rim_joins = jnp.where(behind & joins, their_count, 0.0)
    rim_rows = jnp.sum(rim_joins, axis=0)

    square = (rows, rows)
    line = jnp.broadcast_to(docs, square)
    column = line.T
    here = iota(square, 0)
    there = iota(square, 1)
    together = (line == column) & (there <= here)
    opens = column[:, 0:1] == first_doc
    length = jnp.sum(together.astype(F32), axis=1, keepdims=True) + jnp.where(
        opens, carry_length, 0.0
    )
    values = pool_ref[...]
    rim = rim.astype(BF16)
    position = iota((rows, 16), 0)
    back_by = 16 - iota((rows, 16), 1)
    rim_open = (
        jnp.broadcast_to(opens, (rows, 16))
        & (back_by.astype(F32) <= rim_rows)
    )
    scale = iota((rows, channels), 1) % 4
    total = matmul(together.astype(F32).astype(BF16), values) + jnp.where(opens, carry, 0.0)
    amount = jnp.broadcast_to(length, (rows, channels))
    for k, window in ((0, 2), (1, 8), (2, 16)):
        mask = (together & (there > here - window)).astype(F32).astype(BF16)
        rim_mask = (rim_open & (position + back_by < window)).astype(F32).astype(BF16)
        part = matmul(mask, values) + matmul(rim_mask, rim)
        total = jnp.where(scale == k, part, total)
        amount = jnp.where(scale == k, jnp.minimum(length, float(window)), amount)
    pooled = ((total / amount - values.astype(F32)) * gain_ref[...]).astype(BF16)
    parts = three_parts(norm_ref[...])
    tail = jnp.concatenate([*parts, jnp.zeros((5, 128), F32)], axis=0).astype(BF16)
    for k in range(8):
        both = matmul(pooled, project_ref[:, 256 * k : 256 * (k + 1)])
        for side in (0, 1):
            out_ref[2 * k + side, 0:128] = both[:, 128 * side : 128 * (side + 1)].astype(BF16)
            out_ref[2 * k + side, 128:136] = tail


def sending(arrived_ref, residual_ref, slots_ref, hidden_ref, out_ref, gain_ref):
    projected = jnp.zeros((128, 128), F32)
    for k in range(16):
        projected = projected + arrived_ref[k, 0:128].astype(F32)
        tail = arrived_ref[k, 128:136].astype(F32)
        gain_ref[k : k + 1] = tail[0:1] + tail[1:2] + tail[2:3]
    hidden = residual_ref[...].astype(F32) + projected.astype(BF16).astype(F32)
    hidden_ref[...] = hidden
    slot = iota((512, 128), 0).astype(F32)
    chosen = (slot == slots_ref[0:1]) | (slot == slots_ref[1:2])
    picked = matmul(chosen.astype(F32).astype(BF16), hidden.astype(BF16))
    out_ref[...] = picked.reshape(64, 8, 128).astype(BF16)


def experts(
    core_ref,
    x_ref,
    message_ref,
    gain_ref,
    gate0,
    gate1,
    up0,
    up1,
    down0,
    down1,
    sgate0,
    sgate1,
    sup0,
    sup1,
    sdown0,
    sdown1,
    out_ref,
    normed_ref,
):
    squares = jnp.zeros((256, 128), F32)
    for k in range(16):
        part = x_ref[k // 2, :, k % 2].astype(F32).reshape(256, 128)
        squares = squares + part * part
    scaling = lax.rsqrt(jnp.sum(squares, axis=1, keepdims=True) * (1.0 / 2048.0) + 1e-06)
    for k in range(16):
        part = x_ref[k // 2, :, k % 2].astype(F32).reshape(256, 128)
        normed_ref[:, 128 * k : 128 * (k + 1)] = (part * scaling * gain_ref[k : k + 1]).astype(
            BF16
        )
    message = message_ref[...].astype(F32)
    side = jnp.where(core_ref[0] == 0, message[:, 0:8], message[:, 8:16])
    side = side.reshape(256, 128)
    weight = side[:, W_LANE : W_LANE + 1] + (
        side[:, W_LANE + 1 : W_LANE + 2] + side[:, W_LANE + 2 : W_LANE + 3]
    )
    first = side[:, W_LANE + 3 : W_LANE + 4]
    normed = normed_ref[...]

    def hidden(gate, up, factor):
        upper = matmul(normed, up[...])
        lower = matmul(normed, gate[...])
        return (jax.nn.silu(lower) * upper * factor).astype(BF16)

    pieces = (
        (hidden(gate0, up0, weight), down0),
        (hidden(gate1, up1, weight), down1),
        (hidden(sgate0, sup0, first), sdown0),
        (hidden(sgate1, sup1, first), sdown1),
    )
    for k in range(8):
        cut = slice(256 * k, 256 * (k + 1))
        total = sum(matmul(value, down[:, cut]) for value, down in pieces)
        out_ref[k, :, 0] = total[:, :128].reshape(32, 8, 128).astype(BF16)
        out_ref[k, :, 1] = total[:, 128:].reshape(32, 8, 128).astype(BF16)


def adding(arrived_ref, out_ref):
    total = arrived_ref[0].astype(F32)
    for k in range(1, 8):
        total = total + arrived_ref[k].astype(F32)
    out_ref[...] = total.astype(BF16)


def closing(arrived_ref, slots_ref, hidden_ref, out_ref):
    slot = iota((128, 512), 1).astype(F32)
    first = jnp.broadcast_to(slots_ref[0:1], (128, 128)).T[:, 0:1]
    second = jnp.broadcast_to(slots_ref[1:2], (128, 128)).T[:, 0:1]
    chosen = (slot == first) | (slot == second)
    arrived = arrived_ref[...].astype(F32).reshape(512, 128).astype(BF16)
    routed = matmul(chosen.astype(F32).astype(BF16), arrived)
    out_ref[...] = (hidden_ref[...] + routed).astype(BF16)


VMEM = pl.BlockSpec(memory_space=pltpu.VMEM)
SMEM = pl.BlockSpec(memory_space=pltpu.SMEM)


def kernel(body, name, outs, operands, scalars=0, scratch=()):
    return pl.pallas_call(
        body,
        name=name,
        out_shape=outs,
        in_specs=[SMEM] * scalars + [VMEM] * (len(operands) - scalars),
        out_specs=jax.tree.map(lambda _: VMEM, outs),
        scratch_shapes=scratch,
        compiler_params=pltpu.CompilerParams(vmem_limit_bytes=56 * 2**20),
    )(*operands)


def array(shape, kind):
    return jax.ShapeDtypeStruct(shape, kind)


def body(
    pool_input,
    doc_ids,
    residual,
    pool_gain,
    out_proj,
    norm_gain,
    routes,
    route_weights,
    expert_gate,
    expert_up,
    expert_down,
    shared_gate,
    shared_up,
    shared_down,
):
    docs = doc_ids.reshape(1, 128)
    message, slots = kernel(
        opening,
        "opening",
        (array((32, 16, 128), BF16), array((8, 128), F32)),
        (pool_input, docs, routes, route_weights),
    )
    swap = ((0, 1), (1, 0))
    own = (
        expert_gate[0],
        expert_up[0],
        expert_down[0],
        shared_gate,
        shared_up,
        shared_down,
    )
    other = [lax.ppermute(value, "c", swap) for value in own]
    arrived = exchanged(message, "sp")
    index = lax.axis_index("sp").astype(jnp.int32).reshape(1)
    core = lax.axis_index("c").astype(jnp.int32).reshape(1)
    terms = kernel(
        pooling,
        "pooling",
        array((16, 136, 128), BF16),
        (
            index,
            arrived,
            pool_input,
            docs,
            pool_gain.reshape(1, 64),
            out_proj,
            norm_gain.reshape(1, 128),
        ),
        scalars=1,
    )
    terms = exchanged(terms, ("y", "c"))
    hidden_state, outgoing, gains = kernel(
        sending,
        "sending",
        (array((128, 128), F32), array((64, 8, 128), BF16), array((16, 128), F32)),
        (terms, residual, slots),
    )
    rows = exchanged(outgoing, ("sp", "c"))
    rows = exchanged(jnp.broadcast_to(rows, (8, *rows.shape)), "y")
    pairs = [part for both in zip(own, other) for part in both]
    parts = kernel(
        experts,
        "experts",
        array((8, 32, 2, 8, 128), BF16),
        (core, rows.reshape(8, 32, 2, 8, 128), arrived, gains, *pairs),
        scalars=1,
        scratch=[pltpu.VMEM((256, 2048), BF16)],
    )
    parts = exchanged(parts.reshape(8, 64, 8, 128), "y")
    summed = kernel(adding, "adding", array((64, 8, 128), BF16), (parts,))
    returned = exchanged(summed, ("sp", "c"))
    return kernel(
        closing, "closing", array((128, 128), BF16), (returned, slots, hidden_state)
    )


def solution(mesh):
    split = Mesh(mesh.devices.reshape(32, 8, 2), ("sp", "y", "c"))
    tp = ("y", "c")
    placed = (
        P("sp", tp),
        P("sp"),
        P("sp", tp),
        P(tp),
        P(tp, None),
        P(tp),
        P("sp", None),
        P("sp", None),
        P("sp", None, tp),
        P("sp", None, tp),
        P("sp", tp, None),
        P(None, tp),
        P(None, tp),
        P(tp, None),
    )
    return jax.shard_map(
        body, mesh=split, in_specs=placed, out_specs=P("sp", tp), check_vma=False
    )
```

```python
import jax
import jax.numpy as jnp
from jax import lax
from jax.experimental import pallas as pl
from jax.experimental.pallas import tpu as pltpu
from jax.sharding import Mesh
from jax.sharding import PartitionSpec as P

F32 = jnp.float32
BF16 = jnp.bfloat16
SUM_LANE = 64
W_LANE = 80
META_LANE = 88


def exchanged(value, axis):
    return lax.all_to_all(value, axis, split_axis=0, concat_axis=0, tiled=True)


def three_parts(value):
    first = value.astype(BF16).astype(F32)
    second = (value - first).astype(BF16).astype(F32)
    third = (value - first - second).astype(BF16).astype(F32)
    return first, second, third


def iota(shape, dim):
    return lax.broadcasted_iota(jnp.int32, shape, dim)


def matmul(a, b):
    return jnp.dot(a, b, preferred_element_type=F32)


def opening(pool_ref, docs_ref, routes_ref, weights_ref, message_ref, slots_ref, values_ref):
    channels, rows = pool_ref.shape
    square = (rows, rows)
    values = pool_ref[...].astype(F32).T.astype(BF16)
    values_ref[...] = values
    across = iota((channels, 128), 0)
    lane = iota((channels, 128), 1)
    spread = (lane == across) | ((across % 4 == 3) & (lane == SUM_LANE + across // 4))
    wide = matmul(values, spread.astype(F32).astype(BF16))
    docs = docs_ref[...].astype(F32)
    last_doc = docs[:, rows - 1 :]
    trailing = (docs == last_doc).astype(F32)
    sums = matmul(jnp.broadcast_to(trailing, (8, rows)).astype(BF16), wide.astype(BF16))[0:1]
    count = jnp.sum(trailing, axis=1, keepdims=True)

    lines = [jnp.broadcast_to(routes_ref[k : k + 1].astype(F32), square) for k in (0, 1)]
    columns = [line.T for line in lines]
    before = iota(square, 0) < iota(square, 1)

    def counted(mask):
        return jnp.sum(mask.astype(F32), axis=0, keepdims=True)

    first_rank = counted((columns[0] == lines[0]) & before)
    second_rank = counted(columns[0] == lines[1]) + counted((columns[1] == lines[1]) & before)
    first_slot = lines[0][0:1] * 16.0 + first_rank
    second_slot = lines[1][0:1] * 16.0 + second_rank
    slots_ref[...] = jnp.concatenate(
        [first_slot, second_slot, jnp.zeros((6, rows), F32)], axis=0
    )
    share = [weights_ref[k : k + 1] for k in (0, 1)]
    slot = iota((512, rows), 0).astype(F32)
    is_first = slot == first_slot
    is_second = slot == second_slot
    weight = jnp.sum(
        jnp.where(is_first, share[0], 0.0) + jnp.where(is_second, share[1], 0.0),
        axis=1,
        keepdims=True,
    )
    chosen_first = jnp.sum(is_first.astype(F32), axis=1, keepdims=True)

    row = iota((16, 128), 0)
    at = iota((16, 128), 1)
    parts = three_parts(sums)
    shared = jnp.where(at < channels, wide[rows - 16 :], 0.0)
    in_sums = (at >= SUM_LANE) & (at < SUM_LANE + 16)
    for k in range(3):
        shared = jnp.where(in_sums & (row == k), parts[k], shared)
    doc_high = jnp.floor(last_doc * (1.0 / 128.0))
    doc_low = last_doc - doc_high * 128.0
    for k, value in enumerate((count, doc_high, doc_low)):
        shared = jnp.where(at == META_LANE + k, value, shared)
    place = iota((512, 128), 1)
    message = jnp.broadcast_to(shared[None], (32, 16, 128)).reshape(512, 128)
    for k, value in enumerate((*three_parts(weight), chosen_first)):
        message = jnp.where(place == W_LANE + k, value, message)
    message_ref[...] = message.reshape(32, 16, 128).astype(BF16)


def pooling(
    index_ref, arrived_ref, pool_ref, docs_ref, gain_ref, project_ref, norm_ref, out_ref
):
    rows, channels = pool_ref.shape
    own = index_ref[0]
    docs = docs_ref[...].astype(F32)
    first_doc = docs[:, 0:1]
    arrived = arrived_ref[...].astype(F32)
    meta = arrived[:, 0:1]
    their_count = meta[:, :, META_LANE : META_LANE + 1]
    their_doc = (
        meta[:, :, META_LANE + 1 : META_LANE + 2] * 128.0
        + meta[:, :, META_LANE + 2 : META_LANE + 3]
    )
    block = iota((32, 1, 1), 0)
    joins = (block < own) & (their_doc == first_doc.reshape(1, 1, 1))
    carry_length = jnp.sum(jnp.where(joins, their_count, 0.0), axis=0)
    sums = jnp.sum(jnp.where(joins, arrived[:, 0:8], 0.0), axis=0)
    sums = jnp.where(iota((8, 128), 0) < 3, sums, 0.0)
    back = (iota((128, channels), 0) == SUM_LANE + iota((128, channels), 1) // 4) & (
        iota((128, channels), 1) % 4 == 3
    )
    total = jnp.sum(sums, axis=0, keepdims=True)
    carry = sum(
        matmul(jnp.broadcast_to(part, (8, 128)).astype(BF16), back.astype(F32).astype(BF16))
        for part in three_parts(total)
    )[0:1]

    behind = block == own - 1
    rim = jnp.sum(jnp.where(behind, arrived, 0.0), axis=0)[:, :channels]
    rim_joins = jnp.where(behind & joins, their_count, 0.0)
    rim_rows = jnp.sum(rim_joins, axis=0)

    square = (rows, rows)
    line = jnp.broadcast_to(docs, square)
    column = line.T
    here = iota(square, 0)
    there = iota(square, 1)
    together = (line == column) & (there <= here)
    opens = column[:, 0:1] == first_doc
    length = jnp.sum(together.astype(F32), axis=1, keepdims=True) + jnp.where(
        opens, carry_length, 0.0
    )
    values = pool_ref[...]
    rim = rim.astype(BF16)
    position = iota((rows, 16), 0)
    back_by = 16 - iota((rows, 16), 1)
    rim_open = (
        jnp.broadcast_to(opens, (rows, 16))
        & (back_by.astype(F32) <= rim_rows)
    )
    scale = iota((rows, channels), 1) % 4
    total = matmul(together.astype(F32).astype(BF16), values) + jnp.where(opens, carry, 0.0)
    amount = jnp.broadcast_to(length, (rows, channels))
    for k, window in ((0, 2), (1, 8), (2, 16)):
        mask = (together & (there > here - window)).astype(F32).astype(BF16)
        rim_mask = (rim_open & (position + back_by < window)).astype(F32).astype(BF16)
        part = matmul(mask, values) + matmul(rim_mask, rim)
        total = jnp.where(scale == k, part, total)
        amount = jnp.where(scale == k, jnp.minimum(length, float(window)), amount)
    pooled = ((total / amount - values.astype(F32)) * gain_ref[...]).astype(BF16)
    parts = three_parts(norm_ref[...])
    tail = jnp.concatenate([*parts, jnp.zeros((5, 128), F32)], axis=0).astype(BF16)
    for k in range(8):
        both = matmul(pooled, project_ref[:, 256 * k : 256 * (k + 1)])
        for side in (0, 1):
            out_ref[2 * k + side, 0:128] = both[:, 128 * side : 128 * (side + 1)].astype(BF16)
            out_ref[2 * k + side, 128:136] = tail


def sending(arrived_ref, slots_ref, residual_ref, hidden_ref, out_ref, gain_ref):
    projected = jnp.zeros((128, 128), F32)
    for k in range(16):
        projected = projected + arrived_ref[k, 0:128].astype(F32)
        tail = arrived_ref[k, 128:136].astype(F32)
        gain_ref[k : k + 1] = tail[0:1] + tail[1:2] + tail[2:3]
    hidden = residual_ref[...].astype(F32) + projected.astype(BF16).astype(F32)
    hidden_ref[...] = hidden
    slot = iota((512, 128), 0).astype(F32)
    chosen = (slot == slots_ref[0:1]) | (slot == slots_ref[1:2])
    picked = matmul(chosen.astype(F32).astype(BF16), hidden.astype(BF16))
    out_ref[...] = picked.reshape(64, 8, 128).astype(BF16)


def spreading(arrived_ref, out_ref):
    for k in range(8):
        out_ref[k] = arrived_ref[...]


def experts(core_ref, x_ref, message_ref, gain_ref, *refs):
    sources, out_ref, normed_ref = refs[:12], refs[12], refs[13]
    near, landed = refs[14:26], refs[26]
    copies = [
        pltpu.make_async_copy(source, target, landed.at[k])
        for k, (source, target) in enumerate(zip(sources, near))
    ]
    order = (0, 2, 1, 3, 6, 7, 8, 9, 4, 5, 10, 11)
    for k in order:
        copies[k].start()
    gate0, gate1, up0, up1, down0, down1, sgate0, sgate1, sup0, sup1, sdown0, sdown1 = near

    squares = jnp.zeros((256, 128), F32)
    for k in range(16):
        part = x_ref[k // 2, :, k % 2].astype(F32).reshape(256, 128)
        squares = squares + part * part
    scaling = lax.rsqrt(jnp.sum(squares, axis=1, keepdims=True) * (1.0 / 2048.0) + 1e-06)
    for k in range(16):
        part = x_ref[k // 2, :, k % 2].astype(F32).reshape(256, 128)
        normed_ref[:, 128 * k : 128 * (k + 1)] = (part * scaling * gain_ref[k : k + 1]).astype(
            BF16
        )
    message = message_ref[...].astype(F32)
    side = jnp.where(core_ref[0] == 0, message[:, 0:8], message[:, 8:16])
    side = side.reshape(256, 128)
    weight = side[:, W_LANE : W_LANE + 1] + (
        side[:, W_LANE + 1 : W_LANE + 2] + side[:, W_LANE + 2 : W_LANE + 3]
    )
    first = side[:, W_LANE + 3 : W_LANE + 4]
    normed = normed_ref[...]

    def hidden(gate, up, factor):
        upper = matmul(normed, up[...])
        lower = matmul(normed, gate[...])
        return (jax.nn.silu(lower) * upper * factor).astype(BF16)

    copies[0].wait()
    copies[2].wait()
    left = hidden(gate0, up0, weight)
    copies[1].wait()
    copies[3].wait()
    right = hidden(gate1, up1, weight)
    for k in (6, 7, 8, 9):
        copies[k].wait()
    across = jnp.concatenate([sgate0[...], sgate1[...], sup0[...], sup1[...]], axis=0)
    both = lax.dot_general(
        normed, across, (((1,), (1,)), ((), ())), preferred_element_type=F32
    )
    shared = (jax.nn.silu(both[:, :128]) * both[:, 128:] * first).astype(BF16)
    for k in (4, 5, 10, 11):
        copies[k].wait()
    sdown = jnp.concatenate([sdown0[...], sdown1[...]], axis=0)
    for k in range(8):
        cut = slice(256 * k, 256 * (k + 1))
        total = matmul(left, down0[:, cut]) + matmul(right, down1[:, cut])
        total = total + matmul(shared, sdown[:, cut])
        out_ref[k, :, 0] = total[:, :128].reshape(32, 8, 128).astype(BF16)
        out_ref[k, :, 1] = total[:, 128:].reshape(32, 8, 128).astype(BF16)


def adding(arrived_ref, out_ref):
    total = arrived_ref[0].astype(F32)
    for k in range(1, 8):
        total = total + arrived_ref[k].astype(F32)
    out_ref[...] = total.astype(BF16)


def closing(arrived_ref, slots_ref, hidden_ref, out_ref):
    slot = iota((128, 512), 1).astype(F32)
    first = jnp.broadcast_to(slots_ref[0:1], (128, 128)).T[:, 0:1]
    second = jnp.broadcast_to(slots_ref[1:2], (128, 128)).T[:, 0:1]
    chosen = (slot == first) | (slot == second)
    arrived = arrived_ref[...].astype(F32).reshape(512, 128).astype(BF16)
    routed = matmul(chosen.astype(F32).astype(BF16), arrived)
    out_ref[...] = (hidden_ref[...] + routed).astype(BF16)


VMEM = pl.BlockSpec(memory_space=pltpu.VMEM)
SMEM = pl.BlockSpec(memory_space=pltpu.SMEM)


HBM = pl.BlockSpec(memory_space=pl.ANY)


def kernel(body, name, outs, operands, near=(), far=(), scalars=0, scratch=(), room=16):
    near = [pltpu.with_memory_space_constraint(value, pltpu.VMEM) for value in near]
    far = [pltpu.with_memory_space_constraint(value, pltpu.HBM) for value in far]
    scalar = operands[:scalars]
    plain = [
        pltpu.with_memory_space_constraint(value, pltpu.HBM) for value in operands[scalars:]
    ]
    return pl.pallas_call(
        body,
        name=name,
        out_shape=outs,
        in_specs=[SMEM] * scalars
        + [VMEM] * (len(near) + len(plain))
        + [HBM] * len(far),
        out_specs=jax.tree.map(lambda _: VMEM, outs),
        scratch_shapes=scratch,
        compiler_params=pltpu.CompilerParams(vmem_limit_bytes=room * 2**20),
    )(*scalar, *near, *plain, *far)


def array(shape, kind):
    return pltpu.VMEM(shape, kind)


def body(
    pool_input,
    doc_ids,
    residual,
    pool_gain,
    out_proj,
    norm_gain,
    routes,
    route_weights,
    expert_gate,
    expert_up,
    expert_down,
    shared_gate,
    shared_up,
    shared_down,
):
    docs = doc_ids.reshape(1, 128)
    message, slots, values = kernel(
        opening,
        "opening",
        (array((32, 16, 128), BF16), array((8, 128), F32), array((128, 64), BF16)),
        (pool_input.T, docs, routes.T, route_weights.T),
    )
    swap = ((0, 1), (1, 0))
    own = (
        expert_gate[0],
        expert_up[0],
        expert_down[0],
        shared_gate.T,
        shared_up.T,
        shared_down,
    )
    other = [lax.ppermute(value, "c", swap) for value in own]
    arrived = exchanged(message, "sp")
    index = lax.axis_index("sp").astype(jnp.int32).reshape(1)
    core = lax.axis_index("c").astype(jnp.int32).reshape(1)
    terms = kernel(
        pooling,
        "pooling",
        array((16, 136, 128), BF16),
        (index, docs, pool_gain.reshape(1, 64), out_proj, norm_gain.reshape(1, 128)),
        near=(arrived, values),
        scalars=1,
    )
    terms = exchanged(terms, ("y", "c"))
    hidden_state, outgoing, gains = kernel(
        sending,
        "sending",
        (array((128, 128), F32), array((64, 8, 128), BF16), array((16, 128), F32)),
        (residual,),
        near=(terms, slots),
    )
    rows = exchanged(outgoing, ("sp", "c"))
    rows = kernel(spreading, "spreading", array((8, 64, 8, 128), BF16), (), near=(rows,))
    rows = exchanged(rows, "y")
    pairs = [part for both in zip(own, other) for part in both]
    parts = kernel(
        experts,
        "experts",
        array((8, 32, 2, 8, 128), BF16),
        (core,),
        near=(rows.reshape(8, 32, 2, 8, 128), arrived, gains),
        far=pairs,
        scalars=1,
        scratch=[pltpu.VMEM((256, 2048), BF16)]
        + [pltpu.VMEM(value.shape, BF16) for value in pairs]
        + [pltpu.SemaphoreType.DMA((len(pairs),))],
        room=24,
    )
    parts = exchanged(parts.reshape(8, 64, 8, 128), "y")
    summed = kernel(adding, "adding", array((64, 8, 128), BF16), (), near=(parts,))
    returned = exchanged(summed, ("sp", "c"))
    return kernel(
        closing,
        "closing",
        jax.ShapeDtypeStruct((128, 128), BF16),
        (),
        near=(returned, slots, hidden_state),
    )


def solution(mesh):
    split = Mesh(mesh.devices.reshape(32, 8, 2), ("sp", "y", "c"))
    tp = ("y", "c")
    placed = (
        P("sp", tp),
        P("sp"),
        P("sp", tp),
        P(tp),
        P(tp, None),
        P(tp),
        P("sp", None),
        P("sp", None),
        P("sp", None, tp),
        P("sp", None, tp),
        P("sp", tp, None),
        P(None, tp),
        P(None, tp),
        P(tp, None),
    )
    return jax.shard_map(
        body, mesh=split, in_specs=placed, out_specs=P("sp", tp), check_vma=False
    )
```

```python
import jax
import jax.numpy as jnp
from jax import lax
from jax.experimental import pallas as pl
from jax.experimental.pallas import tpu as pltpu
from jax.sharding import Mesh
from jax.sharding import PartitionSpec as P


F32 = jnp.float32
BF16 = jnp.bfloat16
SUM_LANE = 64
W_LANE = 80
META_LANE = 88


SWAP = ((0, 1), (1, 0))
AROUND = tuple(
    (2 * y + c, 2 * ((y + (1 if c else -1)) % 8) + c) for y in range(8) for c in range(2)
)


def exchanged(value, axis):
    return lax.all_to_all(value, axis, split_axis=0, concat_axis=0, tiled=True)


def three_parts(value):
    first = value.astype(BF16).astype(F32)
    second = (value - first).astype(BF16).astype(F32)
    third = (value - first - second).astype(BF16).astype(F32)
    return first, second, third


def iota(shape, dim):
    return lax.broadcasted_iota(jnp.int32, shape, dim)


def matmul(a, b):
    return jnp.dot(a, b, preferred_element_type=F32)


def opening(pool_ref, docs_ref, routes_ref, weights_ref, message_ref, slots_ref, values_ref):
    channels, rows = pool_ref.shape
    square = (rows, rows)
    values = pool_ref[...].astype(F32).T.astype(BF16)
    values_ref[...] = values
    across = iota((channels, 128), 0)
    lane = iota((channels, 128), 1)
    spread = (lane == across) | ((across % 4 == 3) & (lane == SUM_LANE + across // 4))
    wide = matmul(values, spread.astype(F32).astype(BF16))
    docs = docs_ref[...].astype(F32)
    last_doc = docs[:, rows - 1 :]
    trailing = (docs == last_doc).astype(F32)
    sums = matmul(jnp.broadcast_to(trailing, (8, rows)).astype(BF16), wide.astype(BF16))[0:1]
    count = jnp.sum(trailing, axis=1, keepdims=True)

    lines = [jnp.broadcast_to(routes_ref[k : k + 1].astype(F32), square) for k in (0, 1)]
    columns = [line.T for line in lines]
    before = iota(square, 0) < iota(square, 1)

    def counted(mask):
        return jnp.sum(mask.astype(F32), axis=0, keepdims=True)

    first_rank = counted((columns[0] == lines[0]) & before)
    second_rank = counted(columns[0] == lines[1]) + counted((columns[1] == lines[1]) & before)
    first_slot = lines[0][0:1] * 16.0 + first_rank
    second_slot = lines[1][0:1] * 16.0 + second_rank
    slots_ref[...] = jnp.concatenate(
        [first_slot, second_slot, jnp.zeros((6, rows), F32)], axis=0
    )
    share = [weights_ref[k : k + 1] for k in (0, 1)]
    slot = iota((512, rows), 0).astype(F32)
    is_first = slot == first_slot
    is_second = slot == second_slot
    weight = jnp.sum(
        jnp.where(is_first, share[0], 0.0) + jnp.where(is_second, share[1], 0.0),
        axis=1,
        keepdims=True,
    )
    chosen_first = jnp.sum(is_first.astype(F32), axis=1, keepdims=True)

    row = iota((16, 128), 0)
    at = iota((16, 128), 1)
    parts = three_parts(sums)
    shared = jnp.where(at < channels, wide[rows - 16 :], 0.0)
    in_sums = (at >= SUM_LANE) & (at < SUM_LANE + 16)
    for k in range(3):
        shared = jnp.where(in_sums & (row == k), parts[k], shared)
    doc_high = jnp.floor(last_doc * (1.0 / 128.0))
    doc_low = last_doc - doc_high * 128.0
    for k, value in enumerate((count, doc_high, doc_low)):
        shared = jnp.where(at == META_LANE + k, value, shared)
    place = iota((512, 128), 1)
    message = jnp.broadcast_to(shared[None], (32, 16, 128)).reshape(512, 128)
    for k, value in enumerate((*three_parts(weight), chosen_first)):
        message = jnp.where(place == W_LANE + k, value, message)
    message_ref[...] = message.reshape(32, 16, 128).astype(BF16)


def pooling(
    index_ref, arrived_ref, pool_ref, docs_ref, gain_ref, project_ref, norm_ref, out_ref
):
    rows, channels = pool_ref.shape
    own = index_ref[0]
    docs = docs_ref[...].astype(F32)
    first_doc = docs[:, 0:1]
    arrived = arrived_ref[...].astype(F32)
    meta = arrived[:, 0:1]
    their_count = meta[:, :, META_LANE : META_LANE + 1]
    their_doc = (
        meta[:, :, META_LANE + 1 : META_LANE + 2] * 128.0
        + meta[:, :, META_LANE + 2 : META_LANE + 3]
    )
    block = iota((32, 1, 1), 0)
    joins = (block < own) & (their_doc == first_doc.reshape(1, 1, 1))
    carry_length = jnp.sum(jnp.where(joins, their_count, 0.0), axis=0)
    sums = jnp.sum(jnp.where(joins, arrived[:, 0:8], 0.0), axis=0)
    sums = jnp.where(iota((8, 128), 0) < 3, sums, 0.0)
    back = (iota((128, channels), 0) == SUM_LANE + iota((128, channels), 1) // 4) & (
        iota((128, channels), 1) % 4 == 3
    )
    total = jnp.sum(sums, axis=0, keepdims=True)
    carry = sum(
        matmul(jnp.broadcast_to(part, (8, 128)).astype(BF16), back.astype(F32).astype(BF16))
        for part in three_parts(total)
    )[0:1]

    behind = block == own - 1
    rim = jnp.sum(jnp.where(behind, arrived, 0.0), axis=0)[:, :channels]
    rim_joins = jnp.where(behind & joins, their_count, 0.0)
    rim_rows = jnp.sum(rim_joins, axis=0)

    square = (rows, rows)
    line = jnp.broadcast_to(docs, square)
    column = line.T
    here = iota(square, 0)
    there = iota(square, 1)
    together = (line == column) & (there <= here)
    opens = column[:, 0:1] == first_doc
    length = jnp.sum(together.astype(F32), axis=1, keepdims=True) + jnp.where(
        opens, carry_length, 0.0
    )
    values = pool_ref[...]
    rim = rim.astype(BF16)
    position = iota((rows, 16), 0)
    back_by = 16 - iota((rows, 16), 1)
    rim_open = (
        jnp.broadcast_to(opens, (rows, 16))
        & (back_by.astype(F32) <= rim_rows)
    )
    scale = iota((rows, channels), 1) % 4
    total = matmul(together.astype(F32).astype(BF16), values) + jnp.where(opens, carry, 0.0)
    amount = jnp.broadcast_to(length, (rows, channels))
    for k, window in ((0, 2), (1, 8), (2, 16)):
        mask = (together & (there > here - window)).astype(F32).astype(BF16)
        rim_mask = (rim_open & (position + back_by < window)).astype(F32).astype(BF16)
        part = matmul(mask, values) + matmul(rim_mask, rim)
        total = jnp.where(scale == k, part, total)
        amount = jnp.where(scale == k, jnp.minimum(length, float(window)), amount)
    pooled = ((total / amount - values.astype(F32)) * gain_ref[...]).astype(BF16)
    parts = three_parts(norm_ref[...])
    tail = jnp.concatenate([*parts, jnp.zeros((5, 128), F32)], axis=0).astype(BF16)
    for k in range(8):
        both = matmul(pooled, project_ref[:, 256 * k : 256 * (k + 1)])
        for side in (0, 1):
            out_ref[2 * k + side, 0:128] = both[:, 128 * side : 128 * (side + 1)].astype(BF16)
            out_ref[2 * k + side, 128:136] = tail


def sending(arrived_ref, slots_ref, residual_ref, hidden_ref, out_ref, gain_ref):
    projected = jnp.zeros((128, 128), F32)
    for k in range(16):
        projected = projected + arrived_ref[k, 0:128].astype(F32)
        tail = arrived_ref[k, 128:136].astype(F32)
        gain_ref[k : k + 1] = tail[0:1] + tail[1:2] + tail[2:3]
    hidden = residual_ref[...].astype(F32) + projected.astype(BF16).astype(F32)
    hidden_ref[...] = hidden
    slot = iota((512, 128), 0).astype(F32)
    chosen = (slot == slots_ref[0:1]) | (slot == slots_ref[1:2])
    picked = matmul(chosen.astype(F32).astype(BF16), hidden.astype(BF16))
    out_ref[...] = picked.reshape(64, 8, 128).astype(BF16)


def spreading(arrived_ref, out_ref):
    for k in range(8):
        out_ref[k] = arrived_ref[:, k % 2]


def experts(place_ref, x_ref, message_ref, gain_ref, *refs):
    sources, out_ref, normed_ref = refs[:16], refs[16], refs[17]
    near, landed = refs[18:34], refs[34]
    copies = [
        pltpu.make_async_copy(source, target, landed.at[k])
        for k, (source, target) in enumerate(zip(sources, near))
    ]
    gates, ups, downs, packs = (near[4 * k : 4 * k + 4] for k in range(4))
    for k in range(4):
        copies[k].start()
        copies[4 + k].start()
    for k in (12, 13, 14, 15, 8, 9, 10, 11):
        copies[k].start()

    squares = jnp.zeros((128, 128), F32)
    for k in range(16):
        part = x_ref[k // 2, :, k % 2].astype(F32).reshape(128, 128)
        squares = squares + part * part
    scaling = lax.rsqrt(jnp.sum(squares, axis=1, keepdims=True) * (1.0 / 2048.0) + 1e-06)
    for k in range(16):
        part = x_ref[k // 2, :, k % 2].astype(F32).reshape(128, 128)
        normed_ref[:, 128 * k : 128 * (k + 1)] = (part * scaling * gain_ref[k : k + 1]).astype(
            BF16
        )
    message = message_ref[...].astype(F32).reshape(16, 2, 16, 128)
    message = jnp.where(place_ref[1] == 0, message[:, 0], message[:, 1])
    side = jnp.where(place_ref[0] == 0, message[:, 0:8], message[:, 8:16])
    side = side.reshape(128, 128)
    weight = side[:, W_LANE : W_LANE + 1] + (
        side[:, W_LANE + 1 : W_LANE + 2] + side[:, W_LANE + 2 : W_LANE + 3]
    )
    first = side[:, W_LANE + 3 : W_LANE + 4]
    normed = normed_ref[...]
    hidden = []
    for k in range(4):
        copies[k].wait()
        copies[4 + k].wait()
        lower = matmul(normed, gates[k][...])
        upper = matmul(normed, ups[k][...])
        hidden.append((jax.nn.silu(lower) * upper * weight).astype(BF16))
    for k in range(12, 16):
        copies[k].wait()
    across = jnp.concatenate(
        [pack[0:64] for pack in packs] + [pack[64:128] for pack in packs], axis=0
    )
    both = lax.dot_general(
        normed, across, (((1,), (1,)), ((), ())), preferred_element_type=F32
    )
    shared = (jax.nn.silu(both[:, :256]) * both[:, 256:] * first).astype(BF16)
    for k in range(8, 12):
        copies[k].wait()
    shared_down = jnp.concatenate([pack[128:192] for pack in packs], axis=0)
    for k in range(8):
        cut = slice(256 * k, 256 * (k + 1))
        total = matmul(shared, shared_down[:, cut])
        for value, down in zip(hidden, downs):
            total = total + matmul(value, down[:, cut])
        out_ref[k, :, 0] = total[:, :128].reshape(16, 8, 128).astype(BF16)
        out_ref[k, :, 1] = total[:, 128:].reshape(16, 8, 128).astype(BF16)


def adding(arrived_ref, out_ref):
    for side in (0, 1):
        total = arrived_ref[side].astype(F32)
        for k in range(2 + side, 8, 2):
            total = total + arrived_ref[k].astype(F32)
        out_ref[:, side] = total.astype(BF16)


def closing(arrived_ref, slots_ref, hidden_ref, out_ref):
    slot = iota((128, 512), 1).astype(F32)
    first = jnp.broadcast_to(slots_ref[0:1], (128, 128)).T[:, 0:1]
    second = jnp.broadcast_to(slots_ref[1:2], (128, 128)).T[:, 0:1]
    chosen = (slot == first) | (slot == second)
    arrived = arrived_ref[...].astype(F32).reshape(512, 128).astype(BF16)
    routed = matmul(chosen.astype(F32).astype(BF16), arrived)
    out_ref[...] = (hidden_ref[...] + routed).astype(BF16)


VMEM = pl.BlockSpec(memory_space=pltpu.VMEM)
SMEM = pl.BlockSpec(memory_space=pltpu.SMEM)


HBM = pl.BlockSpec(memory_space=pl.ANY)


def kernel(body, outs, operands, near=(), far=(), scalars=0, scratch=(), room=16):
    near = [pltpu.with_memory_space_constraint(value, pltpu.VMEM) for value in near]
    far = [pltpu.with_memory_space_constraint(value, pltpu.HBM) for value in far]
    scalar = operands[:scalars]
    plain = [
        pltpu.with_memory_space_constraint(value, pltpu.HBM) for value in operands[scalars:]
    ]
    return pl.pallas_call(
        body,
        out_shape=outs,
        in_specs=[SMEM] * scalars
        + [VMEM] * (len(near) + len(plain))
        + [HBM] * len(far),
        out_specs=jax.tree.map(lambda _: VMEM, outs),
        scratch_shapes=scratch,
        compiler_params=pltpu.CompilerParams(vmem_limit_bytes=room * 2**20),
    )(*scalar, *near, *plain, *far)


def array(shape, kind):
    return pltpu.VMEM(shape, kind)


def body(
    pool_input,
    doc_ids,
    residual,
    pool_gain,
    out_proj,
    norm_gain,
    routes,
    route_weights,
    expert_gate,
    expert_up,
    expert_down,
    shared_gate,
    shared_up,
    shared_down,
):
    docs = doc_ids.reshape(1, 128)
    own = {
        "gate": expert_gate[0],
        "up": expert_up[0],
        "down": expert_down[0],
    }
    own["shared"] = jnp.concatenate([shared_gate.T, shared_up.T, shared_down], axis=0)
    ring, own_other, ring_other = {}, {}, {}
    for name, value in own.items():
        ring[name] = lax.ppermute(value, ("y", "c"), AROUND)
        own_other[name] = lax.ppermute(value, "c", SWAP)
        ring_other[name] = lax.ppermute(ring[name], "c", SWAP)

    message, slots, values = kernel(
        opening,
        (array((32, 16, 128), BF16), array((8, 128), F32), array((128, 64), BF16)),
        (pool_input.T, docs, routes.T, route_weights.T),
    )
    arrived = exchanged(message, "sp")
    index = lax.axis_index("sp").astype(jnp.int32).reshape(1)
    terms = kernel(
        pooling,
        array((16, 136, 128), BF16),
        (index, docs, pool_gain.reshape(1, 64), out_proj, norm_gain.reshape(1, 128)),
        near=(arrived, values),
        scalars=1,
    )
    terms = exchanged(terms, ("y", "c"))
    hidden_state, outgoing, gains = kernel(
        sending,
        (array((128, 128), F32), array((64, 8, 128), BF16), array((16, 128), F32)),
        (residual,),
        near=(terms, slots),
    )
    rows = exchanged(outgoing, ("sp", "c"))
    rows = kernel(
        spreading, array((8, 16, 2, 8, 128), BF16), (), near=(rows.reshape(16, 2, 2, 8, 128),)
    )
    rows = exchanged(rows, "y")
    place = jnp.stack([lax.axis_index("c"), lax.axis_index("y") & 1]).astype(jnp.int32)
    groups = [
        part
        for name in own
        for part in (own[name], own_other[name], ring[name], ring_other[name])
    ]
    parts = kernel(
        experts,
        array((8, 16, 2, 8, 128), BF16),
        (place,),
        near=(rows, arrived, gains),
        far=groups,
        scalars=1,
        scratch=[pltpu.VMEM((128, 2048), BF16)]
        + [pltpu.VMEM(value.shape, BF16) for value in groups]
        + [pltpu.SemaphoreType.DMA((len(groups),))],
        room=32,
    )
    parts = exchanged(parts, "y")
    summed = kernel(adding, array((16, 2, 2, 8, 128), BF16), (), near=(parts,))
    returned = exchanged(summed.reshape(64, 8, 128), ("sp", "c"))
    return kernel(
        closing, jax.ShapeDtypeStruct((128, 128), BF16), (), near=(returned, slots, hidden_state)
    )


def solution(mesh):
    split = Mesh(mesh.devices.reshape(32, 8, 2), ("sp", "y", "c"))
    tp = ("y", "c")
    placed = (
        P("sp", tp),
        P("sp"),
        P("sp", tp),
        P(tp),
        P(tp, None),
        P(tp),
        P("sp", None),
        P("sp", None),
        P("sp", None, tp),
        P("sp", None, tp),
        P("sp", tp, None),
        P(None, tp),
        P(None, tp),
        P(tp, None),
    )
    return jax.shard_map(body, mesh=split, in_specs=placed, out_specs=P("sp", tp), check_vma=False)
```

```python
import jax
import jax.numpy as jnp
from jax import lax
from jax.experimental import pallas as pl
from jax.experimental.pallas import tpu as pltpu
from jax.sharding import Mesh
from jax.sharding import PartitionSpec as P


F32 = jnp.float32
BF16 = jnp.bfloat16
SUM_LANE = 64
W_LANE = 80
META_LANE = 88


SWAP = ((0, 1), (1, 0))
AROUND = tuple(
    (2 * y + c, 2 * ((y + (1 if c else -1)) % 8) + c) for y in range(8) for c in range(2)
)


def exchanged(value, axis):
    return lax.all_to_all(value, axis, split_axis=0, concat_axis=0, tiled=True)


def three_parts(value):
    first = value.astype(BF16).astype(F32)
    second = (value - first).astype(BF16).astype(F32)
    third = (value - first - second).astype(BF16).astype(F32)
    return first, second, third


def iota(shape, dim):
    return lax.broadcasted_iota(jnp.int32, shape, dim)


def matmul(a, b):
    return jnp.dot(a, b, preferred_element_type=F32)


def opening(
    pool_ref,
    docs_ref,
    routes_ref,
    weights_ref,
    gate_ref,
    up_ref,
    message_ref,
    slots_ref,
    values_ref,
    pack_ref,
    packed,
):
    copies = [
        pltpu.make_async_copy(source, pack_ref.at[k], packed.at[k])
        for k, source in enumerate((gate_ref, up_ref))
    ]
    for copy in copies:
        copy.start()
    channels, rows = pool_ref.shape
    square = (rows, rows)
    values = pool_ref[...].astype(F32).T.astype(BF16)
    values_ref[...] = values
    across = iota((channels, 128), 0)
    lane = iota((channels, 128), 1)
    spread = (lane == across) | ((across % 4 == 3) & (lane == SUM_LANE + across // 4))
    wide = matmul(values, spread.astype(F32).astype(BF16))
    docs = docs_ref[...].astype(F32)
    last_doc = docs[:, rows - 1 :]
    trailing = (docs == last_doc).astype(F32)
    sums = matmul(jnp.broadcast_to(trailing, (8, rows)).astype(BF16), wide.astype(BF16))[0:1]
    count = jnp.sum(trailing, axis=1, keepdims=True)

    lines = [jnp.broadcast_to(routes_ref[k : k + 1].astype(F32), square) for k in (0, 1)]
    columns = [line.T for line in lines]
    before = iota(square, 0) < iota(square, 1)

    def counted(mask):
        return jnp.sum(mask.astype(F32), axis=0, keepdims=True)

    first_rank = counted((columns[0] == lines[0]) & before)
    second_rank = counted(columns[0] == lines[1]) + counted((columns[1] == lines[1]) & before)
    first_slot = lines[0][0:1] * 16.0 + first_rank
    second_slot = lines[1][0:1] * 16.0 + second_rank
    slots_ref[...] = jnp.concatenate(
        [first_slot, second_slot, jnp.zeros((6, rows), F32)], axis=0
    )
    share = [weights_ref[k : k + 1] for k in (0, 1)]
    slot = iota((512, rows), 0).astype(F32)
    is_first = slot == first_slot
    is_second = slot == second_slot
    weight = jnp.sum(
        jnp.where(is_first, share[0], 0.0) + jnp.where(is_second, share[1], 0.0),
        axis=1,
        keepdims=True,
    )
    chosen_first = jnp.sum(is_first.astype(F32), axis=1, keepdims=True)

    row = iota((16, 128), 0)
    at = iota((16, 128), 1)
    parts = three_parts(sums)
    shared = jnp.where(at < channels, wide[rows - 16 :], 0.0)
    in_sums = (at >= SUM_LANE) & (at < SUM_LANE + 16)
    for k in range(3):
        shared = jnp.where(in_sums & (row == k), parts[k], shared)
    doc_high = jnp.floor(last_doc * (1.0 / 128.0))
    doc_low = last_doc - doc_high * 128.0
    for k, value in enumerate((count, doc_high, doc_low)):
        shared = jnp.where(at == META_LANE + k, value, shared)
    place = iota((512, 128), 1)
    message = jnp.broadcast_to(shared[None], (32, 16, 128)).reshape(512, 128)
    for k, value in enumerate((*three_parts(weight), chosen_first)):
        message = jnp.where(place == W_LANE + k, value, message)
    message_ref[...] = message.reshape(32, 16, 128).astype(BF16)
    for copy in copies:
        copy.wait()


def packing(*refs):
    sources, pack_ref, packed = refs[:4], refs[4], refs[5]
    copies, start = [], 0
    for k, source in enumerate(sources):
        rows = source.shape[0]
        copies.append(
            pltpu.make_async_copy(source, pack_ref.at[start : start + rows], packed.at[k])
        )
        copies[-1].start()
        start += rows
    for copy in copies:
        copy.wait()


def pooling(
    index_ref, arrived_ref, pool_ref, docs_ref, gain_ref, project_ref, norm_ref, out_ref
):
    rows, channels = pool_ref.shape
    own = index_ref[0]
    docs = docs_ref[...].astype(F32)
    first_doc = docs[:, 0:1]
    arrived = arrived_ref[...].astype(F32)
    meta = arrived[:, 0:1]
    their_count = meta[:, :, META_LANE : META_LANE + 1]
    their_doc = (
        meta[:, :, META_LANE + 1 : META_LANE + 2] * 128.0
        + meta[:, :, META_LANE + 2 : META_LANE + 3]
    )
    block = iota((32, 1, 1), 0)
    joins = (block < own) & (their_doc == first_doc.reshape(1, 1, 1))
    carry_length = jnp.sum(jnp.where(joins, their_count, 0.0), axis=0)
    sums = jnp.sum(jnp.where(joins, arrived[:, 0:8], 0.0), axis=0)
    sums = jnp.where(iota((8, 128), 0) < 3, sums, 0.0)
    back = (iota((128, channels), 0) == SUM_LANE + iota((128, channels), 1) // 4) & (
        iota((128, channels), 1) % 4 == 3
    )
    total = jnp.sum(sums, axis=0, keepdims=True)
    carry = sum(
        matmul(jnp.broadcast_to(part, (8, 128)).astype(BF16), back.astype(F32).astype(BF16))
        for part in three_parts(total)
    )[0:1]

    behind = block == own - 1
    rim = jnp.sum(jnp.where(behind, arrived, 0.0), axis=0)[:, :channels]
    rim_joins = jnp.where(behind & joins, their_count, 0.0)
    rim_rows = jnp.sum(rim_joins, axis=0)

    square = (rows, rows)
    line = jnp.broadcast_to(docs, square)
    column = line.T
    here = iota(square, 0)
    there = iota(square, 1)
    together = (line == column) & (there <= here)
    opens = column[:, 0:1] == first_doc
    length = jnp.sum(together.astype(F32), axis=1, keepdims=True) + jnp.where(
        opens, carry_length, 0.0
    )
    values = pool_ref[...]
    rim = rim.astype(BF16)
    position = iota((rows, 16), 0)
    back_by = 16 - iota((rows, 16), 1)
    rim_open = (
        jnp.broadcast_to(opens, (rows, 16))
        & (back_by.astype(F32) <= rim_rows)
    )
    scale = iota((rows, channels), 1) % 4
    total = matmul(together.astype(F32).astype(BF16), values) + jnp.where(opens, carry, 0.0)
    amount = jnp.broadcast_to(length, (rows, channels))
    for k, window in ((0, 2), (1, 8), (2, 16)):
        mask = (together & (there > here - window)).astype(F32).astype(BF16)
        rim_mask = (rim_open & (position + back_by < window)).astype(F32).astype(BF16)
        part = matmul(mask, values) + matmul(rim_mask, rim)
        total = jnp.where(scale == k, part, total)
        amount = jnp.where(scale == k, jnp.minimum(length, float(window)), amount)
    pooled = ((total / amount - values.astype(F32)) * gain_ref[...]).astype(BF16)
    parts = three_parts(norm_ref[...])
    tail = jnp.concatenate([*parts, jnp.zeros((5, 128), F32)], axis=0).astype(BF16)
    for k in range(8):
        both = matmul(pooled, project_ref[:, 256 * k : 256 * (k + 1)])
        for side in (0, 1):
            out_ref[2 * k + side, 0:128] = both[:, 128 * side : 128 * (side + 1)].astype(BF16)
            out_ref[2 * k + side, 128:136] = tail


def sending(arrived_ref, slots_ref, residual_ref, hidden_ref, out_ref, gain_ref):
    projected = jnp.zeros((128, 128), F32)
    for k in range(16):
        projected = projected + arrived_ref[k, 0:128].astype(F32)
        tail = arrived_ref[k, 128:136].astype(F32)
        gain_ref[k : k + 1] = tail[0:1] + tail[1:2] + tail[2:3]
    hidden = residual_ref[...].astype(F32) + projected.astype(BF16).astype(F32)
    hidden_ref[...] = hidden
    slot = iota((512, 128), 0).astype(F32)
    chosen = (slot == slots_ref[0:1]) | (slot == slots_ref[1:2])
    picked = matmul(chosen.astype(F32).astype(BF16), hidden.astype(BF16))
    out_ref[...] = picked.reshape(64, 8, 128).astype(BF16)


def spreading(arrived_ref, out_ref):
    for k in range(8):
        out_ref[k] = arrived_ref[:, k % 2]


def experts(place_ref, x_ref, message_ref, gain_ref, *refs):
    sources, out_ref, normed_ref = refs[:8], refs[8], refs[9]
    near, landed = refs[10:18], refs[18]
    copies = [
        pltpu.make_async_copy(source, target, landed.at[k])
        for k, (source, target) in enumerate(zip(sources, near))
    ]
    for copy in copies[:2]:
        copy.start()
    uppers, lowers = near[:4], near[4:]

    squares = jnp.zeros((128, 128), F32)
    for k in range(16):
        part = x_ref[k // 2, :, k % 2].astype(F32).reshape(128, 128)
        squares = squares + part * part
    scaling = lax.rsqrt(jnp.sum(squares, axis=1, keepdims=True) * (1.0 / 2048.0) + 1e-06)
    for k in range(16):
        part = x_ref[k // 2, :, k % 2].astype(F32).reshape(128, 128)
        normed_ref[:, 128 * k : 128 * (k + 1)] = (part * scaling * gain_ref[k : k + 1]).astype(
            BF16
        )
    message = message_ref[...].astype(F32).reshape(16, 2, 16, 128)
    message = jnp.where(place_ref[1] == 0, message[:, 0], message[:, 1])
    side = jnp.where(place_ref[0] == 0, message[:, 0:8], message[:, 8:16])
    side = side.reshape(128, 128)
    weight = side[:, W_LANE : W_LANE + 1] + (
        side[:, W_LANE + 1 : W_LANE + 2] + side[:, W_LANE + 2 : W_LANE + 3]
    )
    first = side[:, W_LANE + 3 : W_LANE + 4]
    normed = normed_ref[...]
    hidden = []
    for k in range(4):
        copies[k].wait()
        copies[k + 2].start()
        if k == 3:
            copies[6].start()
            copies[7].start()
        lower = matmul(normed, uppers[k][0])
        upper = matmul(normed, uppers[k][1])
        hidden.append((jax.nn.silu(lower) * upper * weight).astype(BF16))
    for copy in copies[4:]:
        copy.wait()
    across = jnp.concatenate(
        [pack[256:320] for pack in lowers] + [pack[320:384] for pack in lowers], axis=0
    )
    both = lax.dot_general(
        normed, across, (((1,), (1,)), ((), ())), preferred_element_type=F32
    )
    shared = (jax.nn.silu(both[:, :256]) * both[:, 256:] * first).astype(BF16)
    shared_down = jnp.concatenate([pack[384:448] for pack in lowers], axis=0)
    for k in range(8):
        cut = slice(256 * k, 256 * (k + 1))
        total = matmul(shared, shared_down[:, cut])
        for value, pack in zip(hidden, lowers):
            total = total + matmul(value, pack[0:256, cut])
        out_ref[k, :, 0] = total[:, :128].reshape(16, 8, 128).astype(BF16)
        out_ref[k, :, 1] = total[:, 128:].reshape(16, 8, 128).astype(BF16)


def adding(arrived_ref, out_ref):
    for side in (0, 1):
        total = arrived_ref[side].astype(F32)
        for k in range(2 + side, 8, 2):
            total = total + arrived_ref[k].astype(F32)
        out_ref[:, side] = total.astype(BF16)


def closing(arrived_ref, slots_ref, hidden_ref, out_ref):
    slot = iota((128, 512), 1).astype(F32)
    first = jnp.broadcast_to(slots_ref[0:1], (128, 128)).T[:, 0:1]
    second = jnp.broadcast_to(slots_ref[1:2], (128, 128)).T[:, 0:1]
    chosen = (slot == first) | (slot == second)
    arrived = arrived_ref[...].astype(F32).reshape(512, 128).astype(BF16)
    routed = matmul(chosen.astype(F32).astype(BF16), arrived)
    out_ref[...] = (hidden_ref[...] + routed).astype(BF16)


VMEM = pl.BlockSpec(memory_space=pltpu.VMEM)
SMEM = pl.BlockSpec(memory_space=pltpu.SMEM)


HBM = pl.BlockSpec(memory_space=pl.ANY)


def is_array(value):
    return not isinstance(value, tuple)


def spec_of(value):
    far = getattr(value, "memory_space", None) == pltpu.HBM
    return HBM if far else VMEM


def kernel(body, outs, operands, near=(), far=(), scalars=0, scratch=(), room=16):
    near = [pltpu.with_memory_space_constraint(value, pltpu.VMEM) for value in near]
    far = [pltpu.with_memory_space_constraint(value, pltpu.HBM) for value in far]
    scalar = operands[:scalars]
    plain = [
        pltpu.with_memory_space_constraint(value, pltpu.HBM) for value in operands[scalars:]
    ]
    return pl.pallas_call(
        body,
        out_shape=outs,
        in_specs=[SMEM] * scalars
        + [VMEM] * (len(near) + len(plain))
        + [HBM] * len(far),
        out_specs=jax.tree.map(spec_of, outs, is_leaf=is_array),
        scratch_shapes=scratch,
        compiler_params=pltpu.CompilerParams(vmem_limit_bytes=room * 2**20),
    )(*scalar, *near, *plain, *far)


def array(shape, kind):
    return pltpu.VMEM(shape, kind)


def body(
    pool_input,
    doc_ids,
    residual,
    pool_gain,
    out_proj,
    norm_gain,
    routes,
    route_weights,
    expert_gate,
    expert_up,
    expert_down,
    shared_gate,
    shared_up,
    shared_down,
):
    docs = doc_ids.reshape(1, 128)
    message, slots, values, upper = kernel(
        opening,
        (
            array((32, 16, 128), BF16),
            array((8, 128), F32),
            array((128, 64), BF16),
            pltpu.HBM((2, 2048, 256), BF16),
        ),
        (pool_input.T, docs, routes.T, route_weights.T),
        far=(expert_gate[0], expert_up[0]),
        scratch=[pltpu.SemaphoreType.DMA((2,))],
    )
    lower = kernel(
        packing,
        pltpu.HBM((448, 2048), BF16),
        (),
        far=(expert_down[0], shared_gate.T, shared_up.T, shared_down),
        scratch=[pltpu.SemaphoreType.DMA((4,))],
    )
    uppers, lowers = [upper], [lower]
    for group in (uppers, lowers):
        value = group[0]
        ring = lax.ppermute(value, ("y", "c"), AROUND)
        own_other = lax.ppermute(value, "c", SWAP)
        ring_other = lax.ppermute(ring, "c", SWAP)
        group += [own_other, ring, ring_other]
    arrived = exchanged(message, "sp")
    index = lax.axis_index("sp").astype(jnp.int32).reshape(1)
    terms = kernel(
        pooling,
        array((16, 136, 128), BF16),
        (index, docs, pool_gain.reshape(1, 64), out_proj, norm_gain.reshape(1, 128)),
        near=(arrived, values),
        scalars=1,
    )
    terms = exchanged(terms, ("y", "c"))
    hidden_state, outgoing, gains = kernel(
        sending,
        (array((128, 128), F32), array((64, 8, 128), BF16), array((16, 128), F32)),
        (residual,),
        near=(terms, slots),
    )
    rows = exchanged(outgoing, ("sp", "c"))
    rows = kernel(
        spreading, array((8, 16, 2, 8, 128), BF16), (), near=(rows.reshape(16, 2, 2, 8, 128),)
    )
    rows = exchanged(rows, "y")
    place = jnp.stack([lax.axis_index("c"), lax.axis_index("y") & 1]).astype(jnp.int32)
    groups = uppers + lowers
    parts = kernel(
        experts,
        array((8, 16, 2, 8, 128), BF16),
        (place,),
        near=(rows, arrived, gains),
        far=groups,
        scalars=1,
        scratch=[pltpu.VMEM((128, 2048), BF16)]
        + [pltpu.VMEM(value.shape, BF16) for value in groups]
        + [pltpu.SemaphoreType.DMA((8,))],
        room=24,
    )
    parts = exchanged(parts, "y")
    summed = kernel(adding, array((16, 2, 2, 8, 128), BF16), (), near=(parts,))
    returned = exchanged(summed.reshape(64, 8, 128), ("sp", "c"))
    return kernel(
        closing, jax.ShapeDtypeStruct((128, 128), BF16), (), near=(returned, slots, hidden_state)
    )


def solution(mesh):
    split = Mesh(mesh.devices.reshape(32, 8, 2), ("sp", "y", "c"))
    tp = ("y", "c")
    placed = (
        P("sp", tp),
        P("sp"),
        P("sp", tp),
        P(tp),
        P(tp, None),
        P(tp),
        P("sp", None),
        P("sp", None),
        P("sp", None, tp),
        P("sp", None, tp),
        P("sp", tp, None),
        P(None, tp),
        P(None, tp),
        P(tp, None),
    )
    return jax.shard_map(body, mesh=split, in_specs=placed, out_specs=P("sp", tp), check_vma=False)
```

```python
import jax
import jax.numpy as jnp
from jax import lax
from jax.experimental import pallas as pl
from jax.experimental.pallas import tpu as pltpu
from jax.sharding import Mesh
from jax.sharding import PartitionSpec as P


F32 = jnp.float32
BF16 = jnp.bfloat16
SUM_LANE = 64
W_LANE = 80
META_LANE = 88


SWAP = ((0, 1), (1, 0))
AROUND = tuple(
    (2 * y + c, 2 * ((y + (1 if c else -1)) % 8) + c) for y in range(8) for c in range(2)
)


def exchanged(value, axis):
    return lax.all_to_all(value, axis, split_axis=0, concat_axis=0, tiled=True)


def three_parts(value):
    first = value.astype(BF16).astype(F32)
    second = (value - first).astype(BF16).astype(F32)
    third = (value - first - second).astype(BF16).astype(F32)
    return first, second, third


def iota(shape, dim):
    return lax.broadcasted_iota(jnp.int32, shape, dim)


def matmul(a, b):
    return jnp.dot(a, b, preferred_element_type=F32)


def opening(
    pool_ref,
    docs_ref,
    routes_ref,
    weights_ref,
    gate_ref,
    up_ref,
    message_ref,
    slots_ref,
    values_ref,
    pack_ref,
    packed,
):
    copies = [
        pltpu.make_async_copy(source, pack_ref.at[k], packed.at[k])
        for k, source in enumerate((gate_ref, up_ref))
    ]
    for copy in copies:
        copy.start()
    channels, rows = pool_ref.shape
    square = (rows, rows)
    values = pool_ref[...].astype(F32).T.astype(BF16)
    values_ref[...] = values
    across = iota((channels, 128), 0)
    lane = iota((channels, 128), 1)
    spread = (lane == across) | ((across % 4 == 3) & (lane == SUM_LANE + across // 4))
    wide = matmul(values, spread.astype(F32).astype(BF16))
    docs = docs_ref[...].astype(F32)
    last_doc = docs[:, rows - 1 :]
    trailing = (docs == last_doc).astype(F32)
    sums = matmul(jnp.broadcast_to(trailing, (8, rows)).astype(BF16), wide.astype(BF16))[0:1]
    count = jnp.sum(trailing, axis=1, keepdims=True)

    lines = [jnp.broadcast_to(routes_ref[k : k + 1].astype(F32), square) for k in (0, 1)]
    columns = [line.T for line in lines]
    before = iota(square, 0) < iota(square, 1)

    def counted(mask):
        return jnp.sum(mask.astype(F32), axis=0, keepdims=True)

    first_rank = counted((columns[0] == lines[0]) & before)
    second_rank = counted(columns[0] == lines[1]) + counted((columns[1] == lines[1]) & before)
    first_slot = lines[0][0:1] * 16.0 + first_rank
    second_slot = lines[1][0:1] * 16.0 + second_rank
    slots_ref[...] = jnp.concatenate(
        [first_slot, second_slot, jnp.zeros((6, rows), F32)], axis=0
    )
    share = [weights_ref[k : k + 1] for k in (0, 1)]
    slot = iota((512, rows), 0).astype(F32)
    is_first = slot == first_slot
    is_second = slot == second_slot
    weight = jnp.sum(
        jnp.where(is_first, share[0], 0.0) + jnp.where(is_second, share[1], 0.0),
        axis=1,
        keepdims=True,
    )
    chosen_first = jnp.sum(is_first.astype(F32), axis=1, keepdims=True)

    row = iota((16, 128), 0)
    at = iota((16, 128), 1)
    parts = three_parts(sums)
    shared = jnp.where(at < channels, wide[rows - 16 :], 0.0)
    in_sums = (at >= SUM_LANE) & (at < SUM_LANE + 16)
    for k in range(3):
        shared = jnp.where(in_sums & (row == k), parts[k], shared)
    doc_high = jnp.floor(last_doc * (1.0 / 128.0))
    doc_low = last_doc - doc_high * 128.0
    for k, value in enumerate((count, doc_high, doc_low)):
        shared = jnp.where(at == META_LANE + k, value, shared)
    place = iota((512, 128), 1)
    message = jnp.broadcast_to(shared[None], (32, 16, 128)).reshape(512, 128)
    for k, value in enumerate((*three_parts(weight), chosen_first)):
        message = jnp.where(place == W_LANE + k, value, message)
    message_ref[...] = message.reshape(32, 16, 128).astype(BF16)
    for copy in copies:
        copy.wait()


def packing(*refs):
    sources, pack_ref, packed = refs[:4], refs[4], refs[5]
    copies, start = [], 0
    for k, source in enumerate(sources):
        rows = source.shape[0]
        copies.append(
            pltpu.make_async_copy(source, pack_ref.at[start : start + rows], packed.at[k])
        )
        copies[-1].start()
        start += rows
    for copy in copies:
        copy.wait()


def pooling(
    index_ref,
    arrived_ref,
    pool_ref,
    docs_ref,
    gain_ref,
    project_ref,
    norm_ref,
    kept_ref,
    out_ref,
):
    rows, channels = pool_ref.shape
    own = index_ref[0]
    docs = docs_ref[...].astype(F32)
    first_doc = docs[:, 0:1]
    arrived = arrived_ref[...].astype(F32)
    meta = arrived[:, 0:1]
    their_count = meta[:, :, META_LANE : META_LANE + 1]
    their_doc = (
        meta[:, :, META_LANE + 1 : META_LANE + 2] * 128.0
        + meta[:, :, META_LANE + 2 : META_LANE + 3]
    )
    block = iota((32, 1, 1), 0)
    joins = (block < own) & (their_doc == first_doc.reshape(1, 1, 1))
    carry_length = jnp.sum(jnp.where(joins, their_count, 0.0), axis=0)
    sums = jnp.sum(jnp.where(joins, arrived[:, 0:8], 0.0), axis=0)
    sums = jnp.where(iota((8, 128), 0) < 3, sums, 0.0)
    back = (iota((128, channels), 0) == SUM_LANE + iota((128, channels), 1) // 4) & (
        iota((128, channels), 1) % 4 == 3
    )
    total = jnp.sum(sums, axis=0, keepdims=True)
    carry = sum(
        matmul(jnp.broadcast_to(part, (8, 128)).astype(BF16), back.astype(F32).astype(BF16))
        for part in three_parts(total)
    )[0:1]

    behind = block == own - 1
    rim = jnp.sum(jnp.where(behind, arrived, 0.0), axis=0)[:, :channels]
    rim_joins = jnp.where(behind & joins, their_count, 0.0)
    rim_rows = jnp.sum(rim_joins, axis=0)

    square = (rows, rows)
    line = jnp.broadcast_to(docs, square)
    column = line.T
    here = iota(square, 0)
    there = iota(square, 1)
    together = (line == column) & (there <= here)
    opens = column[:, 0:1] == first_doc
    length = jnp.sum(together.astype(F32), axis=1, keepdims=True) + jnp.where(
        opens, carry_length, 0.0
    )
    values = pool_ref[...]
    rim = rim.astype(BF16)
    position = iota((rows, 16), 0)
    back_by = 16 - iota((rows, 16), 1)
    rim_open = (
        jnp.broadcast_to(opens, (rows, 16))
        & (back_by.astype(F32) <= rim_rows)
    )
    scale = iota((rows, channels), 1) % 4
    total = matmul(together.astype(F32).astype(BF16), values) + jnp.where(opens, carry, 0.0)
    amount = jnp.broadcast_to(length, (rows, channels))
    for k, window in ((0, 2), (1, 8), (2, 16)):
        mask = (together & (there > here - window)).astype(F32).astype(BF16)
        rim_mask = (rim_open & (position + back_by < window)).astype(F32).astype(BF16)
        part = matmul(mask, values) + matmul(rim_mask, rim)
        total = jnp.where(scale == k, part, total)
        amount = jnp.where(scale == k, jnp.minimum(length, float(window)), amount)
    pooled = ((total / amount - values.astype(F32)) * gain_ref[...]).astype(BF16)
    parts = three_parts(norm_ref[...])
    tail = jnp.concatenate([*parts, jnp.zeros((5, 128), F32)], axis=0).astype(BF16)
    for k in range(8):
        both = matmul(pooled, project_ref[:, 256 * k : 256 * (k + 1)])
        left, right = both[:, :128], both[:, 128:]
        kept_ref[k] = jnp.where(index_ref[1] == 0, left, right)
        out_ref[k, 0:128] = jnp.where(index_ref[1] == 0, right, left).astype(BF16)
        out_ref[k, 128:136] = tail


def pairing(core_ref, kept_ref, arrived_ref, norm_ref, out_ref):
    own = jnp.concatenate([*three_parts(norm_ref[...]), jnp.zeros((5, 128), F32)], axis=0)
    other = arrived_ref[0, 128:136].astype(F32)
    first = core_ref[0] == 0
    tail = jnp.concatenate(
        [
            jnp.where(first, own, other)[0:3],
            jnp.where(first, other, own)[0:3],
            jnp.zeros((2, 128), F32),
        ],
        axis=0,
    ).astype(BF16)
    for k in range(8):
        out_ref[k, 0:128] = (kept_ref[k] + arrived_ref[k, 0:128].astype(F32)).astype(BF16)
        out_ref[k, 128:136] = tail


def sending(arrived_ref, slots_ref, residual_ref, hidden_ref, out_ref, gain_ref):
    projected = jnp.zeros((128, 128), F32)
    for k in range(8):
        projected = projected + arrived_ref[k, 0:128].astype(F32)
        tail = arrived_ref[k, 128:136].astype(F32)
        for side in (0, 1):
            part = tail[3 * side : 3 * side + 3]
            gain_ref[2 * k + side : 2 * k + side + 1] = part[0:1] + part[1:2] + part[2:3]
    hidden = residual_ref[...].astype(F32) + projected.astype(BF16).astype(F32)
    hidden_ref[...] = hidden
    slot = iota((512, 128), 0).astype(F32)
    chosen = (slot == slots_ref[0:1]) | (slot == slots_ref[1:2])
    picked = matmul(chosen.astype(F32).astype(BF16), hidden.astype(BF16))
    out_ref[...] = picked.reshape(64, 8, 128).astype(BF16)


def spreading(arrived_ref, out_ref):
    for k in range(8):
        out_ref[k] = arrived_ref[:, k % 2]


def experts(place_ref, x_ref, message_ref, gain_ref, *refs):
    sources, out_ref, normed_ref = refs[:8], refs[8], refs[9]
    near, landed = refs[10:18], refs[18]
    copies = [
        pltpu.make_async_copy(source, target, landed.at[k])
        for k, (source, target) in enumerate(zip(sources, near))
    ]
    for copy in copies:
        copy.start()
    uppers, lowers = near[:4], near[4:]

    squares = jnp.zeros((128, 128), F32)
    for k in range(16):
        part = x_ref[k // 2, :, k % 2].astype(F32).reshape(128, 128)
        squares = squares + part * part
    scaling = lax.rsqrt(jnp.sum(squares, axis=1, keepdims=True) * (1.0 / 2048.0) + 1e-06)
    for k in range(16):
        part = x_ref[k // 2, :, k % 2].astype(F32).reshape(128, 128)
        normed_ref[:, 128 * k : 128 * (k + 1)] = (part * scaling * gain_ref[k : k + 1]).astype(
            BF16
        )
    message = message_ref[...].astype(F32).reshape(16, 2, 16, 128)
    message = jnp.where(place_ref[1] == 0, message[:, 0], message[:, 1])
    side = jnp.where(place_ref[0] == 0, message[:, 0:8], message[:, 8:16])
    side = side.reshape(128, 128)
    weight = side[:, W_LANE : W_LANE + 1] + (
        side[:, W_LANE + 1 : W_LANE + 2] + side[:, W_LANE + 2 : W_LANE + 3]
    )
    first = side[:, W_LANE + 3 : W_LANE + 4]
    normed = normed_ref[...]
    hidden = []
    for k in range(4):
        copies[k].wait()
        lower = matmul(normed, uppers[k][0])
        upper = matmul(normed, uppers[k][1])
        hidden.append((jax.nn.silu(lower) * upper * weight).astype(BF16))
    for copy in copies[4:]:
        copy.wait()
    across = jnp.concatenate(
        [pack[256:320] for pack in lowers] + [pack[320:384] for pack in lowers], axis=0
    )
    both = lax.dot_general(
        normed, across, (((1,), (1,)), ((), ())), preferred_element_type=F32
    )
    shared = (jax.nn.silu(both[:, :256]) * both[:, 256:] * first).astype(BF16)
    shared_down = jnp.concatenate([pack[384:448] for pack in lowers], axis=0)
    for k in range(8):
        cut = slice(256 * k, 256 * (k + 1))
        total = matmul(shared, shared_down[:, cut])
        for value, pack in zip(hidden, lowers):
            total = total + matmul(value, pack[0:256, cut])
        out_ref[k, :, 0] = total[:, :128].reshape(16, 8, 128).astype(BF16)
        out_ref[k, :, 1] = total[:, 128:].reshape(16, 8, 128).astype(BF16)


def adding(arrived_ref, out_ref):
    for side in (0, 1):
        total = arrived_ref[side].astype(F32)
        for k in range(2 + side, 8, 2):
            total = total + arrived_ref[k].astype(F32)
        out_ref[:, side] = total.astype(BF16)


def closing(arrived_ref, slots_ref, hidden_ref, out_ref):
    slot = iota((128, 512), 1).astype(F32)
    first = jnp.broadcast_to(slots_ref[0:1], (128, 128)).T[:, 0:1]
    second = jnp.broadcast_to(slots_ref[1:2], (128, 128)).T[:, 0:1]
    chosen = (slot == first) | (slot == second)
    arrived = arrived_ref[...].astype(F32).reshape(512, 128).astype(BF16)
    routed = matmul(chosen.astype(F32).astype(BF16), arrived)
    out_ref[...] = (hidden_ref[...] + routed).astype(BF16)


VMEM = pl.BlockSpec(memory_space=pltpu.VMEM)
SMEM = pl.BlockSpec(memory_space=pltpu.SMEM)


HBM = pl.BlockSpec(memory_space=pl.ANY)


def is_array(value):
    return not isinstance(value, tuple)


def spec_of(value):
    far = getattr(value, "memory_space", None) == pltpu.HBM
    return HBM if far else VMEM


def kernel(body, outs, operands, near=(), far=(), scalars=0, scratch=(), room=16):
    near = [pltpu.with_memory_space_constraint(value, pltpu.VMEM) for value in near]
    far = [pltpu.with_memory_space_constraint(value, pltpu.HBM) for value in far]
    scalar = operands[:scalars]
    plain = [
        pltpu.with_memory_space_constraint(value, pltpu.HBM) for value in operands[scalars:]
    ]
    return pl.pallas_call(
        body,
        out_shape=outs,
        in_specs=[SMEM] * scalars
        + [VMEM] * (len(near) + len(plain))
        + [HBM] * len(far),
        out_specs=jax.tree.map(spec_of, outs, is_leaf=is_array),
        scratch_shapes=scratch,
        compiler_params=pltpu.CompilerParams(vmem_limit_bytes=room * 2**20),
    )(*scalar, *near, *plain, *far)


def array(shape, kind):
    return pltpu.VMEM(shape, kind)


def body(
    pool_input,
    doc_ids,
    residual,
    pool_gain,
    out_proj,
    norm_gain,
    routes,
    route_weights,
    expert_gate,
    expert_up,
    expert_down,
    shared_gate,
    shared_up,
    shared_down,
):
    docs = doc_ids.reshape(1, 128)
    message, slots, values, upper = kernel(
        opening,
        (
            array((32, 16, 128), BF16),
            array((8, 128), F32),
            array((128, 64), BF16),
            array((2, 2048, 256), BF16),
        ),
        (pool_input.T, docs, routes.T, route_weights.T),
        far=(expert_gate[0], expert_up[0]),
        scratch=[pltpu.SemaphoreType.DMA((2,))],
    )
    lower = kernel(
        packing,
        array((448, 2048), BF16),
        (),
        far=(expert_down[0], shared_gate.T, shared_up.T, shared_down),
        scratch=[pltpu.SemaphoreType.DMA((4,))],
    )
    uppers, lowers = [upper], [lower]
    for group in (uppers, lowers):
        value = group[0]
        ring = lax.ppermute(value, ("y", "c"), AROUND)
        own_other = lax.ppermute(value, "c", SWAP)
        ring_other = lax.ppermute(ring, "c", SWAP)
        group += [own_other, ring, ring_other]
    arrived = exchanged(message, "sp")
    core = lax.axis_index("c").astype(jnp.int32)
    index = jnp.stack([lax.axis_index("sp").astype(jnp.int32), core])
    kept, terms = kernel(
        pooling,
        (array((8, 128, 128), F32), array((8, 136, 128), BF16)),
        (index, docs, pool_gain.reshape(1, 64), out_proj, norm_gain.reshape(1, 128)),
        near=(arrived, values),
        scalars=1,
    )
    terms = lax.ppermute(terms, "c", SWAP)
    terms = kernel(
        pairing,
        array((8, 136, 128), BF16),
        (core.reshape(1), norm_gain.reshape(1, 128)),
        near=(kept, terms),
        scalars=1,
    )
    terms = exchanged(terms, "y")
    hidden_state, outgoing, gains = kernel(
        sending,
        (array((128, 128), F32), array((64, 8, 128), BF16), array((16, 128), F32)),
        (residual,),
        near=(terms, slots),
    )
    rows = exchanged(outgoing, ("sp", "c"))
    rows = kernel(
        spreading, array((8, 16, 2, 8, 128), BF16), (), near=(rows.reshape(16, 2, 2, 8, 128),)
    )
    rows = exchanged(rows, "y")
    place = jnp.stack([core, lax.axis_index("y").astype(jnp.int32) & 1])
    groups = uppers + lowers
    parts = kernel(
        experts,
        array((8, 16, 2, 8, 128), BF16),
        (place,),
        near=(rows, arrived, gains),
        far=groups,
        scalars=1,
        scratch=[pltpu.VMEM((128, 2048), BF16)]
        + [pltpu.VMEM(value.shape, BF16) for value in groups]
        + [pltpu.SemaphoreType.DMA((8,))],
        room=24,
    )
    parts = exchanged(parts, "y")
    summed = kernel(adding, array((16, 2, 2, 8, 128), BF16), (), near=(parts,))
    returned = exchanged(summed.reshape(64, 8, 128), ("sp", "c"))
    return kernel(
        closing, jax.ShapeDtypeStruct((128, 128), BF16), (), near=(returned, slots, hidden_state)
    )


def solution(mesh):
    split = Mesh(mesh.devices.reshape(32, 8, 2), ("sp", "y", "c"))
    tp = ("y", "c")
    placed = (
        P("sp", tp),
        P("sp"),
        P("sp", tp),
        P(tp),
        P(tp, None),
        P(tp),
        P("sp", None),
        P("sp", None),
        P("sp", None, tp),
        P("sp", None, tp),
        P("sp", tp, None),
        P(None, tp),
        P(None, tp),
        P(tp, None),
    )
    return jax.shard_map(body, mesh=split, in_specs=placed, out_specs=P("sp", tp), check_vma=False)
```

```python
import jax
import jax.numpy as jnp
from jax import lax
from jax.experimental import pallas as pl
from jax.experimental.pallas import tpu as pltpu
from jax.sharding import Mesh
from jax.sharding import PartitionSpec as P


F32 = jnp.float32
BF16 = jnp.bfloat16
SUM_LANE = 64
W_LANE = 80
META_LANE = 88


SWAP = ((0, 1), (1, 0))
AROUND = tuple(
    (2 * y + c, 2 * ((y + (1 if c else -1)) % 8) + c) for y in range(8) for c in range(2)
)


def exchanged(value, axis):
    return lax.all_to_all(value, axis, split_axis=0, concat_axis=0, tiled=True)


def three_parts(value):
    first = value.astype(BF16).astype(F32)
    second = (value - first).astype(BF16).astype(F32)
    third = (value - first - second).astype(BF16).astype(F32)
    return first, second, third


def iota(shape, dim):
    return lax.broadcasted_iota(jnp.int32, shape, dim)


def matmul(a, b):
    return jnp.dot(a, b, preferred_element_type=F32)


def opening(
    core_ref,
    pool_ref,
    docs_ref,
    routes_ref,
    weights_ref,
    gain_ref,
    norm_ref,
    message_ref,
    slots_ref,
    side_ref,
):
    channels, rows = pool_ref.shape
    square = (rows, rows)
    values = pool_ref[...].astype(F32).T.astype(BF16)
    across = iota((channels, 128), 0)
    lane = iota((channels, 128), 1)
    first_core = core_ref[0] == 0
    moved = (lane == across + jnp.where(first_core, 0, channels)).astype(F32).astype(BF16)
    side_ref[0:128] = matmul(values, moved).astype(BF16)
    gains = jnp.concatenate([*three_parts(gain_ref[...]), jnp.zeros((5, channels), F32)], axis=0)
    gains = matmul(gains.astype(BF16), moved)[0:3]
    norms = jnp.concatenate(three_parts(norm_ref[...]), axis=0)
    zeros = jnp.zeros((3, 128), F32)
    tail = [
        gains,
        jnp.where(first_core, norms, zeros),
        jnp.where(first_core, zeros, norms),
        jnp.zeros((7, 128), F32),
    ]
    side_ref[128:144] = jnp.concatenate(tail, axis=0).astype(BF16)
    spread = (lane == across) | ((across % 4 == 3) & (lane == SUM_LANE + across // 4))
    wide = matmul(values, spread.astype(F32).astype(BF16))
    docs = docs_ref[...].astype(F32)
    last_doc = docs[:, rows - 1 :]
    trailing = (docs == last_doc).astype(F32)
    sums = matmul(jnp.broadcast_to(trailing, (8, rows)).astype(BF16), wide.astype(BF16))[0:1]
    count = jnp.sum(trailing, axis=1, keepdims=True)

    lines = [jnp.broadcast_to(routes_ref[k : k + 1].astype(F32), square) for k in (0, 1)]
    columns = [line.T for line in lines]
    before = iota(square, 0) < iota(square, 1)

    def counted(mask):
        return jnp.sum(mask.astype(F32), axis=0, keepdims=True)

    first_rank = counted((columns[0] == lines[0]) & before)
    second_rank = counted(columns[0] == lines[1]) + counted((columns[1] == lines[1]) & before)
    first_slot = lines[0][0:1] * 16.0 + first_rank
    second_slot = lines[1][0:1] * 16.0 + second_rank
    slots_ref[...] = jnp.concatenate(
        [first_slot, second_slot, jnp.zeros((6, rows), F32)], axis=0
    )
    share = [weights_ref[k : k + 1] for k in (0, 1)]
    slot = iota((512, rows), 0).astype(F32)
    is_first = slot == first_slot
    is_second = slot == second_slot
    weight = jnp.sum(
        jnp.where(is_first, share[0], 0.0) + jnp.where(is_second, share[1], 0.0),
        axis=1,
        keepdims=True,
    )
    chosen_first = jnp.sum(is_first.astype(F32), axis=1, keepdims=True)

    row = iota((16, 128), 0)
    at = iota((16, 128), 1)
    parts = three_parts(sums)
    shared = jnp.where(at < channels, wide[rows - 16 :], 0.0)
    in_sums = (at >= SUM_LANE) & (at < SUM_LANE + 16)
    for k in range(3):
        shared = jnp.where(in_sums & (row == k), parts[k], shared)
    doc_high = jnp.floor(last_doc * (1.0 / 128.0))
    doc_low = last_doc - doc_high * 128.0
    for k, value in enumerate((count, doc_high, doc_low)):
        shared = jnp.where(at == META_LANE + k, value, shared)
    place = iota((512, 128), 1)
    message = jnp.broadcast_to(shared[None], (32, 16, 128)).reshape(512, 128)
    for k, value in enumerate((*three_parts(weight), chosen_first)):
        message = jnp.where(place == W_LANE + k, value, message)
    message = message.reshape(32, 16, 128).astype(BF16)
    message_ref[:, 0] = message
    message_ref[:, 1] = message


def packing(*refs):
    sources, pack_ref, packed = refs[:4], refs[4], refs[5]
    copies, start = [], 0
    for k, source in enumerate(sources):
        rows = source.shape[0]
        copies.append(
            pltpu.make_async_copy(source, pack_ref.at[start : start + rows], packed.at[k])
        )
        copies[-1].start()
        start += rows
    for copy in copies:
        copy.wait()


def pooling(
    index_ref,
    arrived_ref,
    side_ref,
    other_ref,
    project_other_ref,
    docs_ref,
    source_ref,
    out_ref,
    project_ref,
    landed,
):
    copy = pltpu.make_async_copy(source_ref, project_ref, landed.at[0])
    copy.start()
    rows = channels = 128
    own = index_ref[0]
    docs = docs_ref[...].astype(F32)
    first_doc = docs[:, 0:1]
    sides = side_ref[...].astype(F32) + other_ref[...].astype(F32)
    values = sides[0:128].astype(BF16)
    gain = sides[128:129] + (sides[129:130] + sides[130:131])
    meta = arrived_ref[:, 0, 0:8].astype(F32)[:, 0:1]
    their_count = meta[:, :, META_LANE : META_LANE + 1]
    their_doc = (
        meta[:, :, META_LANE + 1 : META_LANE + 2] * 128.0
        + meta[:, :, META_LANE + 2 : META_LANE + 3]
    )
    block = iota((32, 1, 1), 0)
    joins = (block < own) & (their_doc == first_doc.reshape(1, 1, 1))
    behind = block == own - 1
    carry_length = jnp.sum(jnp.where(joins, their_count, 0.0), axis=0)
    source = iota((128, 128), 0)
    target = iota((128, 128), 1)
    carry = jnp.zeros((8, 128), F32)
    rim = jnp.zeros((16, 128), F32)
    for side in (0, 1):
        arrived = arrived_ref[:, side].astype(F32)
        sums = jnp.sum(jnp.where(joins, arrived[:, 0:8], 0.0), axis=0)
        total = jnp.sum(jnp.where(iota((8, 128), 0) < 3, sums, 0.0), axis=0, keepdims=True)
        here = target - 64 * side
        inside = (here >= 0) & (here < 64)
        back = inside & (here % 4 == 3) & (source == SUM_LANE + here // 4)
        back = back.astype(F32).astype(BF16)
        for part in three_parts(total):
            carry = carry + matmul(jnp.broadcast_to(part, (8, 128)).astype(BF16), back)
        their_rim = jnp.sum(jnp.where(behind, arrived, 0.0), axis=0).astype(BF16)
        rim = rim + matmul(their_rim, (inside & (source == here)).astype(F32).astype(BF16))
    carry = carry[0:1]
    rim = rim.astype(BF16)
    rim_rows = jnp.sum(jnp.where(behind & joins, their_count, 0.0), axis=0)

    square = (rows, rows)
    line = jnp.broadcast_to(docs, square)
    column = line.T
    here = iota(square, 0)
    there = iota(square, 1)
    together = (line == column) & (there <= here)
    opens = column[:, 0:1] == first_doc
    length = jnp.sum(together.astype(F32), axis=1, keepdims=True) + jnp.where(
        opens, carry_length, 0.0
    )
    position = iota((rows, 16), 0)
    back_by = 16 - iota((rows, 16), 1)
    rim_open = jnp.broadcast_to(opens, (rows, 16)) & (back_by.astype(F32) <= rim_rows)
    scale = iota((rows, channels), 1) % 4
    total = matmul(together.astype(F32).astype(BF16), values) + jnp.where(opens, carry, 0.0)
    amount = jnp.broadcast_to(length, (rows, channels))
    for k, window in ((0, 2), (1, 8), (2, 16)):
        mask = (together & (there > here - window)).astype(F32).astype(BF16)
        rim_mask = (rim_open & (position + back_by < window)).astype(F32).astype(BF16)
        part = matmul(mask, values) + matmul(rim_mask, rim)
        total = jnp.where(scale == k, part, total)
        amount = jnp.where(scale == k, jnp.minimum(length, float(window)), amount)
    pooled = ((total / amount - sides[0:128]) * gain).astype(BF16)
    first_core = index_ref[1] == 0
    pooled_own = jnp.where(first_core, pooled[:, :64].astype(F32), pooled[:, 64:].astype(F32))
    pooled_other = jnp.where(first_core, pooled[:, 64:].astype(F32), pooled[:, :64].astype(F32))
    pooled_own, pooled_other = pooled_own.astype(BF16), pooled_other.astype(BF16)
    tail = jnp.concatenate([sides[131:137], jnp.zeros((2, 128), F32)], axis=0).astype(BF16)
    copy.wait()
    for k in range(8):
        cut = pl.ds(pl.multiple_of(256 * k + 128 * index_ref[1], 128), 128)
        both = matmul(pooled_own, project_ref[:, cut])
        both = both + matmul(pooled_other, project_other_ref[:, cut])
        out_ref[k, 0:128] = both.astype(BF16)
        out_ref[k, 128:136] = tail


def sending(arrived_ref, slots_ref, residual_ref, hidden_ref, out_ref, gain_ref):
    projected = jnp.zeros((128, 128), F32)
    for k in range(8):
        projected = projected + arrived_ref[k, 0:128].astype(F32)
        tail = arrived_ref[k, 128:136].astype(F32)
        for side in (0, 1):
            part = tail[3 * side : 3 * side + 3]
            gain_ref[2 * k + side : 2 * k + side + 1] = part[0:1] + part[1:2] + part[2:3]
    hidden = residual_ref[...].astype(F32) + projected.astype(BF16).astype(F32)
    hidden_ref[...] = hidden
    slot = iota((512, 128), 0).astype(F32)
    chosen = (slot == slots_ref[0:1]) | (slot == slots_ref[1:2])
    picked = matmul(chosen.astype(F32).astype(BF16), hidden.astype(BF16))
    out_ref[...] = picked.reshape(64, 8, 128).astype(BF16)


def spreading(arrived_ref, out_ref):
    for k in range(8):
        out_ref[k] = arrived_ref[:, k % 2]


def experts(place_ref, x_ref, message_ref, gain_ref, *refs):
    sources, out_ref, normed_ref = refs[:12], refs[12], refs[13]
    near, landed = refs[14:26], refs[26]
    gates, ups, lowers = near[0:4], near[4:8], near[8:12]
    order = (0, 4, 1, 5, 2, 6, 3, 7, 8, 9, 10, 11)
    copies = [
        pltpu.make_async_copy(sources[k], near[k], landed.at[k]) for k in order
    ]
    for copy in copies[:6]:
        copy.start()

    squares = jnp.zeros((128, 128), F32)
    for k in range(16):
        part = x_ref[k // 2, :, k % 2].astype(F32).reshape(128, 128)
        squares = squares + part * part
    scaling = lax.rsqrt(jnp.sum(squares, axis=1, keepdims=True) * (1.0 / 2048.0) + 1e-06)
    for k in range(16):
        part = x_ref[k // 2, :, k % 2].astype(F32).reshape(128, 128)
        normed_ref[:, 128 * k : 128 * (k + 1)] = (part * scaling * gain_ref[k : k + 1]).astype(
            BF16
        )
    message = message_ref[:, 0].astype(F32).reshape(16, 2, 16, 128)
    message = jnp.where(place_ref[1] == 0, message[:, 0], message[:, 1])
    side = jnp.where(place_ref[0] == 0, message[:, 0:8], message[:, 8:16])
    side = side.reshape(128, 128)
    weight = side[:, W_LANE : W_LANE + 1] + (
        side[:, W_LANE + 1 : W_LANE + 2] + side[:, W_LANE + 2 : W_LANE + 3]
    )
    first = side[:, W_LANE + 3 : W_LANE + 4]
    normed = normed_ref[...]
    hidden = []
    for k, (gate, up) in enumerate(zip(gates, ups)):
        copies[2 * k].wait()
        copies[2 * k + 1].wait()
        if k < 3:
            copies[6 + 2 * k].start()
            copies[7 + 2 * k].start()
        lower = matmul(normed, gate[...])
        upper = matmul(normed, up[...])
        hidden.append((jax.nn.silu(lower) * upper * weight).astype(BF16))
    for copy in copies[8:]:
        copy.wait()
    across = jnp.concatenate(
        [pack[256:320] for pack in lowers] + [pack[320:384] for pack in lowers], axis=0
    )
    both = lax.dot_general(
        normed, across, (((1,), (1,)), ((), ())), preferred_element_type=F32
    )
    shared = (jax.nn.silu(both[:, :256]) * both[:, 256:] * first).astype(BF16)
    shared_down = jnp.concatenate([pack[384:448] for pack in lowers], axis=0)
    for k in range(8):
        cut = slice(256 * k, 256 * (k + 1))
        total = matmul(shared, shared_down[:, cut])
        for value, pack in zip(hidden, lowers):
            total = total + matmul(value, pack[0:256, cut])
        out_ref[k, :, 0] = total[:, :128].reshape(16, 8, 128).astype(BF16)
        out_ref[k, :, 1] = total[:, 128:].reshape(16, 8, 128).astype(BF16)


def adding(arrived_ref, out_ref):
    for side in (0, 1):
        total = arrived_ref[side].astype(F32)
        for k in range(2 + side, 8, 2):
            total = total + arrived_ref[k].astype(F32)
        out_ref[:, side] = total.astype(BF16)


def closing(arrived_ref, slots_ref, hidden_ref, out_ref):
    slot = iota((128, 512), 1).astype(F32)
    first = jnp.broadcast_to(slots_ref[0:1], (128, 128)).T[:, 0:1]
    second = jnp.broadcast_to(slots_ref[1:2], (128, 128)).T[:, 0:1]
    chosen = (slot == first) | (slot == second)
    arrived = arrived_ref[...].astype(F32).reshape(512, 128).astype(BF16)
    routed = matmul(chosen.astype(F32).astype(BF16), arrived)
    out_ref[...] = (hidden_ref[...] + routed).astype(BF16)


VMEM = pl.BlockSpec(memory_space=pltpu.VMEM)
SMEM = pl.BlockSpec(memory_space=pltpu.SMEM)


HBM = pl.BlockSpec(memory_space=pl.ANY)


def is_array(value):
    return not isinstance(value, tuple)


def spec_of(value):
    far = getattr(value, "memory_space", None) == pltpu.HBM
    return HBM if far else VMEM


def kernel(body, outs, operands, near=(), far=(), scalars=0, scratch=(), room=16):
    near = [pltpu.with_memory_space_constraint(value, pltpu.VMEM) for value in near]
    far = [pltpu.with_memory_space_constraint(value, pltpu.HBM) for value in far]
    scalar = operands[:scalars]
    plain = [
        pltpu.with_memory_space_constraint(value, pltpu.HBM) for value in operands[scalars:]
    ]
    return pl.pallas_call(
        body,
        out_shape=outs,
        in_specs=[SMEM] * scalars
        + [VMEM] * (len(near) + len(plain))
        + [HBM] * len(far),
        out_specs=jax.tree.map(spec_of, outs, is_leaf=is_array),
        scratch_shapes=scratch,
        compiler_params=pltpu.CompilerParams(vmem_limit_bytes=room * 2**20),
    )(*scalar, *near, *plain, *far)


def array(shape, kind):
    return pltpu.VMEM(shape, kind)


def body(
    pool_input,
    doc_ids,
    residual,
    pool_gain,
    out_proj,
    norm_gain,
    routes,
    route_weights,
    expert_gate,
    expert_up,
    expert_down,
    shared_gate,
    shared_up,
    shared_down,
):
    docs = doc_ids.reshape(1, 128)
    core = lax.axis_index("c").astype(jnp.int32)
    index = jnp.stack([lax.axis_index("sp").astype(jnp.int32), core])
    message, slots, side = kernel(
        opening,
        (array((32, 2, 16, 128), BF16), array((8, 128), F32), array((144, 128), BF16)),
        (
            core.reshape(1),
            pool_input.T,
            docs,
            routes.T,
            route_weights.T,
            pool_gain.reshape(1, 64),
            norm_gain.reshape(1, 128),
        ),
        scalars=1,
    )
    packed = kernel(
        packing,
        array((448, 2048), BF16),
        (),
        far=(expert_down[0], shared_gate.T, shared_up.T, shared_down),
        scratch=[pltpu.SemaphoreType.DMA((4,))],
    )
    groups = []
    for value in (expert_gate[0], expert_up[0], packed):
        ring = lax.ppermute(value, ("y", "c"), AROUND)
        own_other = lax.ppermute(value, "c", SWAP)
        ring_other = lax.ppermute(ring, "c", SWAP)
        groups += [value, own_other, ring, ring_other]
    arrived = exchanged(message.reshape(64, 16, 128), ("sp", "c"))
    arrived = arrived.reshape(32, 2, 16, 128)
    other_side = lax.ppermute(side, "c", SWAP)
    other_project = lax.ppermute(out_proj, "c", SWAP)
    terms = kernel(
        pooling,
        array((8, 136, 128), BF16),
        (index, docs),
        near=(arrived, side, other_side, other_project),
        far=(out_proj,),
        scalars=1,
        scratch=[pltpu.VMEM((64, 2048), BF16), pltpu.SemaphoreType.DMA((1,))],
    )
    terms = exchanged(terms, "y")
    hidden_state, outgoing, gains = kernel(
        sending,
        (array((128, 128), F32), array((64, 8, 128), BF16), array((16, 128), F32)),
        (),
        near=(terms, slots, residual),
    )
    rows = exchanged(outgoing, ("sp", "c"))
    rows = kernel(
        spreading, array((8, 16, 2, 8, 128), BF16), (), near=(rows.reshape(16, 2, 2, 8, 128),)
    )
    rows = exchanged(rows, "y")
    place = jnp.stack([core, lax.axis_index("y").astype(jnp.int32) & 1])
    parts = kernel(
        experts,
        array((8, 16, 2, 8, 128), BF16),
        (place,),
        near=(rows, arrived, gains),
        far=groups,
        scalars=1,
        scratch=[pltpu.VMEM((128, 2048), BF16)]
        + [pltpu.VMEM(value.shape, BF16) for value in groups]
        + [pltpu.SemaphoreType.DMA((12,))],
        room=24,
    )
    parts = exchanged(parts, "y")
    summed = kernel(adding, array((16, 2, 2, 8, 128), BF16), (), near=(parts,))
    returned = exchanged(summed.reshape(64, 8, 128), ("sp", "c"))
    return kernel(
        closing, jax.ShapeDtypeStruct((128, 128), BF16), (), near=(returned, slots, hidden_state)
    )


def solution(mesh):
    split = Mesh(mesh.devices.reshape(32, 8, 2), ("sp", "y", "c"))
    tp = ("y", "c")
    placed = (
        P("sp", tp),
        P("sp"),
        P("sp", tp),
        P(tp),
        P(tp, None),
        P(tp),
        P("sp", None),
        P("sp", None),
        P("sp", None, tp),
        P("sp", None, tp),
        P("sp", tp, None),
        P(None, tp),
        P(None, tp),
        P(tp, None),
    )
    return jax.shard_map(body, mesh=split, in_specs=placed, out_specs=P("sp", tp), check_vma=False)
```

```python
import jax
import jax.numpy as jnp
from jax import lax
from jax.experimental import pallas as pl
from jax.experimental.pallas import tpu as pltpu
from jax.sharding import Mesh
from jax.sharding import PartitionSpec as P


F32 = jnp.float32
BF16 = jnp.bfloat16


SWAP = ((0, 1), (1, 0))
AROUND = tuple(
    (2 * y + c, 2 * ((y + (1 if c else -1)) % 8) + c) for y in range(8) for c in range(2)
)


def exchanged(value, axis):
    return lax.all_to_all(value, axis, split_axis=0, concat_axis=0, tiled=True)


def three_parts(value):
    first = value.astype(BF16).astype(F32)
    second = (value - first).astype(BF16).astype(F32)
    third = (value - first - second).astype(BF16).astype(F32)
    return first, second, third


def iota(shape, dim):
    return lax.broadcasted_iota(jnp.int32, shape, dim)


def matmul(a, b):
    return jnp.dot(a, b, preferred_element_type=F32)


def opening(
    core_ref,
    pool_ref,
    docs_ref,
    routes_ref,
    weights_ref,
    gain_ref,
    norm_ref,
    message_ref,
    slots_ref,
    side_ref,
):
    channels, rows = pool_ref.shape
    square = (rows, rows)
    values = pool_ref[...].astype(F32).T.astype(BF16)
    across = iota((channels, 128), 0)
    lane = iota((channels, 128), 1)
    first_core = core_ref[0] == 0
    moved = (lane == across + jnp.where(first_core, 0, channels)).astype(F32).astype(BF16)
    side_ref[0:128] = matmul(values, moved).astype(BF16)
    gains = jnp.concatenate([*three_parts(gain_ref[...]), jnp.zeros((5, channels), F32)], axis=0)
    gains = matmul(gains.astype(BF16), moved)[0:3]
    norms = jnp.concatenate(three_parts(norm_ref[...]), axis=0)
    zeros = jnp.zeros((3, 128), F32)
    tail = [
        gains,
        jnp.where(first_core, norms, zeros),
        jnp.where(first_core, zeros, norms),
        jnp.zeros((7, 128), F32),
    ]
    side_ref[128:144] = jnp.concatenate(tail, axis=0).astype(BF16)
    low = (lane == across).astype(F32).astype(BF16)
    high = (lane == across + channels).astype(F32).astype(BF16)
    rim = matmul(values[rows - 16 :], low)[0:8] + matmul(values[rows - 16 :], high)[8:16]
    docs = docs_ref[...].astype(F32)
    last_doc = docs[:, rows - 1 :]
    trailing = (docs == last_doc).astype(F32)
    sums = matmul(jnp.broadcast_to(trailing, (8, rows)).astype(BF16), values)
    parts = [matmul(part.astype(BF16), low)[0:1] for part in three_parts(sums)]
    count = jnp.sum(trailing, axis=1, keepdims=True)

    lines = [jnp.broadcast_to(routes_ref[k : k + 1].astype(F32), square) for k in (0, 1)]
    columns = [line.T for line in lines]
    before = iota(square, 0) < iota(square, 1)

    def counted(mask):
        return jnp.sum(mask.astype(F32), axis=0, keepdims=True)

    first_rank = counted((columns[0] == lines[0]) & before)
    second_rank = counted(columns[0] == lines[1]) + counted((columns[1] == lines[1]) & before)
    first_slot = lines[0][0:1] * 16.0 + first_rank
    second_slot = lines[1][0:1] * 16.0 + second_rank
    slots_ref[...] = jnp.concatenate(
        [first_slot, second_slot, jnp.zeros((6, rows), F32)], axis=0
    )
    share = [weights_ref[k : k + 1] for k in (0, 1)]
    line = iota((256, rows), 0)
    row = iota((8, 128), 0)
    at = iota((8, 128), 1)
    in_sums = (at < channels) & (at % 4 == 3)
    for k in range(3):
        rim = jnp.where(in_sums & (row == k), parts[k], rim)
    doc_high = jnp.floor(last_doc * (1.0 / 128.0))
    doc_low = last_doc - doc_high * 128.0
    for k, value in enumerate((count, doc_high, doc_low)):
        rim = jnp.where((row == 3) & (at == 3 + 4 * k), value, rim)
    place = iota((256, 128), 1)
    message = jnp.broadcast_to(rim[None], (32, 8, 128)).reshape(256, 128)
    for half in (0, 1):
        slot = (line // 8 * 16 + line % 8 + 8 * half).astype(F32)
        is_first = slot == first_slot
        is_second = slot == second_slot
        weight = jnp.sum(
            jnp.where(is_first, share[0], 0.0) + jnp.where(is_second, share[1], 0.0),
            axis=1,
            keepdims=True,
        )
        chosen_first = jnp.sum(is_first.astype(F32), axis=1, keepdims=True)
        for k, value in enumerate((*three_parts(weight), chosen_first)):
            message = jnp.where(place == 1 + 4 * k + 16 * half, value, message)
    message = message.reshape(32, 8, 128).astype(BF16)
    message_ref[:, 0] = message
    message_ref[:, 1] = message


def packing(*refs):
    sources, pack_ref, packed = refs[:4], refs[4], refs[5]
    copies, start = [], 0
    for k, source in enumerate(sources):
        rows = source.shape[0]
        copies.append(
            pltpu.make_async_copy(source, pack_ref.at[start : start + rows], packed.at[k])
        )
        copies[-1].start()
        start += rows
    for copy in copies:
        copy.wait()


def pooling(
    index_ref,
    arrived_ref,
    side_ref,
    other_ref,
    project_other_ref,
    docs_ref,
    source_ref,
    out_ref,
    project_ref,
    landed,
):
    copy = pltpu.make_async_copy(source_ref, project_ref, landed.at[0])
    copy.start()
    rows = channels = 128
    own = index_ref[0]
    docs = docs_ref[...].astype(F32)
    first_doc = docs[:, 0:1]
    sides = side_ref[...].astype(F32) + other_ref[...].astype(F32)
    values = sides[0:128].astype(BF16)
    gain = sides[128:129] + (sides[129:130] + sides[130:131])
    meta = arrived_ref[:, 0].astype(F32)[:, 3:4]
    their_count = meta[:, :, 3:4]
    their_doc = meta[:, :, 7:8] * 128.0 + meta[:, :, 11:12]
    block = iota((32, 1, 1), 0)
    joins = (block < own) & (their_doc == first_doc.reshape(1, 1, 1))
    behind = block == own - 1
    carry_length = jnp.sum(jnp.where(joins, their_count, 0.0), axis=0)
    source = iota((128, 128), 0)
    target = iota((128, 128), 1)
    carry = jnp.zeros((8, 128), F32)
    upper_rim = jnp.zeros((8, 128), F32)
    lower_rim = jnp.zeros((8, 128), F32)
    for side in (0, 1):
        arrived = arrived_ref[:, side].astype(F32)
        sums = jnp.sum(jnp.where(joins, arrived, 0.0), axis=0)
        total = jnp.sum(jnp.where(iota((8, 128), 0) < 3, sums, 0.0), axis=0, keepdims=True)
        here = target - 64 * side
        inside = (here >= 0) & (here < 64)
        low = (inside & (source == here)).astype(F32).astype(BF16)
        high = (inside & (source == here + 64)).astype(F32).astype(BF16)
        for part in three_parts(total):
            carry = carry + matmul(jnp.broadcast_to(part, (8, 128)).astype(BF16), low)
        their_rim = jnp.sum(jnp.where(behind, arrived, 0.0), axis=0).astype(BF16)
        upper_rim = upper_rim + matmul(their_rim, low)
        lower_rim = lower_rim + matmul(their_rim, high)
    carry = carry[0:1]
    rim = jnp.concatenate([upper_rim, lower_rim], axis=0).astype(BF16)
    rim_rows = jnp.sum(jnp.where(behind & joins, their_count, 0.0), axis=0)

    square = (rows, rows)
    line = jnp.broadcast_to(docs, square)
    column = line.T
    here = iota(square, 0)
    there = iota(square, 1)
    together = (line == column) & (there <= here)
    opens = column[:, 0:1] == first_doc
    length = jnp.sum(together.astype(F32), axis=1, keepdims=True) + jnp.where(
        opens, carry_length, 0.0
    )
    position = iota((rows, 16), 0)
    back_by = 16 - iota((rows, 16), 1)
    rim_open = jnp.broadcast_to(opens, (rows, 16)) & (back_by.astype(F32) <= rim_rows)
    scale = iota((rows, channels), 1) % 4
    total = matmul(together.astype(F32).astype(BF16), values) + jnp.where(opens, carry, 0.0)
    amount = jnp.broadcast_to(length, (rows, channels))
    for k, window in ((0, 2), (1, 8), (2, 16)):
        mask = (together & (there > here - window)).astype(F32).astype(BF16)
        rim_mask = (rim_open & (position + back_by < window)).astype(F32).astype(BF16)
        part = matmul(mask, values) + matmul(rim_mask, rim)
        total = jnp.where(scale == k, part, total)
        amount = jnp.where(scale == k, jnp.minimum(length, float(window)), amount)
    pooled = ((total / amount - sides[0:128]) * gain).astype(BF16)
    first_core = index_ref[1] == 0
    pooled_own = jnp.where(first_core, pooled[:, :64].astype(F32), pooled[:, 64:].astype(F32))
    pooled_other = jnp.where(first_core, pooled[:, 64:].astype(F32), pooled[:, :64].astype(F32))
    pooled_own, pooled_other = pooled_own.astype(BF16), pooled_other.astype(BF16)
    tail = jnp.concatenate([sides[131:137], jnp.zeros((2, 128), F32)], axis=0).astype(BF16)
    copy.wait()
    for k in range(8):
        cut = pl.ds(pl.multiple_of(256 * k + 128 * index_ref[1], 128), 128)
        both = matmul(pooled_own, project_ref[:, cut])
        both = both + matmul(pooled_other, project_other_ref[:, cut])
        out_ref[k, 0:128] = both.astype(BF16)
        out_ref[k, 128:136] = tail


def sending(arrived_ref, slots_ref, residual_ref, hidden_ref, out_ref, gain_ref):
    projected = jnp.zeros((128, 128), F32)
    for k in range(8):
        projected = projected + arrived_ref[k, 0:128].astype(F32)
        tail = arrived_ref[k, 128:136].astype(F32)
        for side in (0, 1):
            part = tail[3 * side : 3 * side + 3]
            gain_ref[2 * k + side : 2 * k + side + 1] = part[0:1] + part[1:2] + part[2:3]
    hidden = residual_ref[...].astype(F32) + projected.astype(BF16).astype(F32)
    hidden_ref[...] = hidden
    slot = iota((512, 128), 0).astype(F32)
    chosen = (slot == slots_ref[0:1]) | (slot == slots_ref[1:2])
    picked = matmul(chosen.astype(F32).astype(BF16), hidden.astype(BF16))
    out_ref[...] = picked.reshape(64, 8, 128).astype(BF16)


def spreading(arrived_ref, out_ref):
    for k in range(8):
        out_ref[k] = arrived_ref[:, k % 2]


def experts(place_ref, x_ref, message_ref, gain_ref, *refs):
    sources, out_ref, normed_ref, sum_ref = refs[:12], refs[12], refs[13], refs[14]
    near, landed = refs[15:27], refs[27]
    gates, ups, lowers = near[0:4], near[4:8], near[8:12]
    copies = [
        pltpu.make_async_copy(sources[k], near[k], landed.at[k]) for k in range(12)
    ]
    for k in (0, 4, 1, 5, 2, 6, 8, 9, 10, 11, 3, 7):
        copies[k].start()

    squares = jnp.zeros((128, 128), F32)
    for k in range(16):
        part = x_ref[k // 2, :, k % 2].astype(F32).reshape(128, 128)
        squares = squares + part * part
    scaling = lax.rsqrt(jnp.sum(squares, axis=1, keepdims=True) * (1.0 / 2048.0) + 1e-06)
    for k in range(16):
        part = x_ref[k // 2, :, k % 2].astype(F32).reshape(128, 128)
        normed_ref[:, 128 * k : 128 * (k + 1)] = (part * scaling * gain_ref[k : k + 1]).astype(
            BF16
        )
    message = message_ref[:, 0].astype(F32).reshape(16, 2, 8, 128)
    side = jnp.where(place_ref[1] == 0, message[:, 0], message[:, 1]).reshape(128, 128)
    left = place_ref[0] == 0
    told = [jnp.where(left, side[:, k : k + 1], side[:, k + 16 : k + 17]) for k in (1, 5, 9, 13)]
    weight = told[0] + (told[1] + told[2])
    first = told[3]
    normed = normed_ref[...]

    def hidden(k):
        copies[k].wait()
        copies[k + 4].wait()
        lower = matmul(normed, gates[k][...])
        upper = matmul(normed, ups[k][...])
        return (jax.nn.silu(lower) * upper * weight).astype(BF16)

    early = [hidden(k) for k in range(3)]
    for copy in copies[8:]:
        copy.wait()
    across = jnp.concatenate(
        [pack[256:320] for pack in lowers] + [pack[320:384] for pack in lowers], axis=0
    )
    both = lax.dot_general(
        normed, across, (((1,), (1,)), ((), ())), preferred_element_type=F32
    )
    shared = (jax.nn.silu(both[:, :256]) * both[:, 256:] * first).astype(BF16)
    shared_down = jnp.concatenate([pack[384:448] for pack in lowers], axis=0)
    for k in range(8):
        cut = slice(256 * k, 256 * (k + 1))
        total = matmul(shared, shared_down[:, cut])
        for value, pack in zip(early, lowers):
            total = total + matmul(value, pack[0:256, cut])
        sum_ref[k] = total
    last = hidden(3)
    for k in range(8):
        cut = slice(256 * k, 256 * (k + 1))
        total = sum_ref[k] + matmul(last, lowers[3][0:256, cut])
        out_ref[k, :, 0] = total[:, :128].reshape(16, 8, 128).astype(BF16)
        out_ref[k, :, 1] = total[:, 128:].reshape(16, 8, 128).astype(BF16)


def adding(arrived_ref, out_ref):
    for side in (0, 1):
        total = arrived_ref[side].astype(F32)
        for k in range(2 + side, 8, 2):
            total = total + arrived_ref[k].astype(F32)
        out_ref[:, side] = total.astype(BF16)


def closing(arrived_ref, slots_ref, hidden_ref, out_ref):
    slot = iota((128, 512), 1).astype(F32)
    first = jnp.broadcast_to(slots_ref[0:1], (128, 128)).T[:, 0:1]
    second = jnp.broadcast_to(slots_ref[1:2], (128, 128)).T[:, 0:1]
    chosen = (slot == first) | (slot == second)
    arrived = arrived_ref[...].astype(F32).reshape(512, 128).astype(BF16)
    routed = matmul(chosen.astype(F32).astype(BF16), arrived)
    out_ref[...] = (hidden_ref[...] + routed).astype(BF16)


VMEM = pl.BlockSpec(memory_space=pltpu.VMEM)
SMEM = pl.BlockSpec(memory_space=pltpu.SMEM)


HBM = pl.BlockSpec(memory_space=pl.ANY)


def is_array(value):
    return not isinstance(value, tuple)


def spec_of(value):
    far = getattr(value, "memory_space", None) == pltpu.HBM
    return HBM if far else VMEM


def kernel(body, outs, operands, near=(), far=(), scalars=0, scratch=(), room=16):
    near = [pltpu.with_memory_space_constraint(value, pltpu.VMEM) for value in near]
    far = [pltpu.with_memory_space_constraint(value, pltpu.HBM) for value in far]
    scalar = operands[:scalars]
    plain = [
        pltpu.with_memory_space_constraint(value, pltpu.HBM) for value in operands[scalars:]
    ]
    return pl.pallas_call(
        body,
        out_shape=outs,
        in_specs=[SMEM] * scalars
        + [VMEM] * (len(near) + len(plain))
        + [HBM] * len(far),
        out_specs=jax.tree.map(spec_of, outs, is_leaf=is_array),
        scratch_shapes=scratch,
        compiler_params=pltpu.CompilerParams(vmem_limit_bytes=room * 2**20),
    )(*scalar, *near, *plain, *far)


def array(shape, kind):
    return pltpu.VMEM(shape, kind)


def body(
    pool_input,
    doc_ids,
    residual,
    pool_gain,
    out_proj,
    norm_gain,
    routes,
    route_weights,
    expert_gate,
    expert_up,
    expert_down,
    shared_gate,
    shared_up,
    shared_down,
):
    docs = doc_ids.reshape(1, 128)
    core = lax.axis_index("c").astype(jnp.int32)
    index = jnp.stack([lax.axis_index("sp").astype(jnp.int32), core])
    message, slots, side = kernel(
        opening,
        (array((32, 2, 8, 128), BF16), array((8, 128), F32), array((144, 128), BF16)),
        (
            core.reshape(1),
            pool_input.T,
            docs,
            routes.T,
            route_weights.T,
            pool_gain.reshape(1, 64),
            norm_gain.reshape(1, 128),
        ),
        scalars=1,
    )
    packed = kernel(
        packing,
        array((448, 2048), BF16),
        (),
        far=(expert_down[0], shared_gate.T, shared_up.T, shared_down),
        scratch=[pltpu.SemaphoreType.DMA((4,))],
    )
    groups = []
    for value in (expert_gate[0], expert_up[0], packed):
        ring = lax.ppermute(value, ("y", "c"), AROUND)
        own_other = lax.ppermute(value, "c", SWAP)
        ring_other = lax.ppermute(ring, "c", SWAP)
        groups += [value, own_other, ring, ring_other]
    arrived = exchanged(message.reshape(64, 8, 128), ("sp", "c"))
    arrived = arrived.reshape(32, 2, 8, 128)
    other_side = lax.ppermute(side, "c", SWAP)
    other_project = lax.ppermute(out_proj, "c", SWAP)
    terms = kernel(
        pooling,
        array((8, 136, 128), BF16),
        (index, docs),
        near=(arrived, side, other_side, other_project),
        far=(out_proj,),
        scalars=1,
        scratch=[pltpu.VMEM((64, 2048), BF16), pltpu.SemaphoreType.DMA((1,))],
    )
    terms = exchanged(terms, "y")
    hidden_state, outgoing, gains = kernel(
        sending,
        (array((128, 128), F32), array((64, 8, 128), BF16), array((16, 128), F32)),
        (),
        near=(terms, slots, residual),
    )
    rows = exchanged(outgoing, ("sp", "c"))
    rows = kernel(
        spreading, array((8, 16, 2, 8, 128), BF16), (), near=(rows.reshape(16, 2, 2, 8, 128),)
    )
    rows = exchanged(rows, "y")
    place = jnp.stack([core, lax.axis_index("y").astype(jnp.int32) & 1])
    parts = kernel(
        experts,
        array((8, 16, 2, 8, 128), BF16),
        (place,),
        near=(rows, arrived, gains),
        far=groups,
        scalars=1,
        scratch=[pltpu.VMEM((128, 2048), BF16), pltpu.VMEM((8, 128, 256), F32)]
        + [pltpu.VMEM(value.shape, BF16) for value in groups]
        + [pltpu.SemaphoreType.DMA((12,))],
        room=24,
    )
    parts = exchanged(parts, "y")
    summed = kernel(adding, array((16, 2, 2, 8, 128), BF16), (), near=(parts,))
    returned = exchanged(summed.reshape(64, 8, 128), ("sp", "c"))
    return kernel(
        closing, jax.ShapeDtypeStruct((128, 128), BF16), (), near=(returned, slots, hidden_state)
    )


def solution(mesh):
    split = Mesh(mesh.devices.reshape(32, 8, 2), ("sp", "y", "c"))
    tp = ("y", "c")
    placed = (
        P("sp", tp),
        P("sp"),
        P("sp", tp),
        P(tp),
        P(tp, None),
        P(tp),
        P("sp", None),
        P("sp", None),
        P("sp", None, tp),
        P("sp", None, tp),
        P("sp", tp, None),
        P(None, tp),
        P(None, tp),
        P(tp, None),
    )
    return jax.shard_map(body, mesh=split, in_specs=placed, out_specs=P("sp", tp), check_vma=False)
```

```python
import jax
import jax.numpy as jnp
from jax import lax
from jax.experimental import pallas as pl
from jax.experimental.pallas import tpu as pltpu
from jax.sharding import Mesh
from jax.sharding import PartitionSpec as P


F32 = jnp.float32
BF16 = jnp.bfloat16


SWAP = ((0, 1), (1, 0))
AROUND = tuple(
    (2 * y + c, 2 * ((y + (1 if c else -1)) % 8) + c) for y in range(8) for c in range(2)
)


def exchanged(value, axis):
    return lax.all_to_all(value, axis, split_axis=0, concat_axis=0, tiled=True)


def three_parts(value):
    first = value.astype(BF16).astype(F32)
    second = (value - first).astype(BF16).astype(F32)
    third = (value - first - second).astype(BF16).astype(F32)
    return first, second, third


def iota(shape, dim):
    return lax.broadcasted_iota(jnp.int32, shape, dim)


def matmul(a, b):
    return jnp.dot(a, b, preferred_element_type=F32)


def opening(
    core_ref,
    pool_ref,
    docs_ref,
    routes_ref,
    weights_ref,
    gain_ref,
    norm_ref,
    source_ref,
    message_ref,
    slots_ref,
    side_ref,
    mine_ref,
    project_ref,
    landed,
):
    copy = pltpu.make_async_copy(source_ref, project_ref, landed.at[0])
    copy.start()
    channels, rows = pool_ref.shape
    square = (rows, rows)
    values = pool_ref[...].astype(F32).T.astype(BF16)
    across = iota((channels, 128), 0)
    lane = iota((channels, 128), 1)
    first_core = core_ref[0] == 0
    moved = (lane == across + jnp.where(first_core, 0, channels)).astype(F32).astype(BF16)
    side_ref[0:128] = matmul(values, moved).astype(BF16)
    gains = jnp.concatenate([*three_parts(gain_ref[...]), jnp.zeros((5, channels), F32)], axis=0)
    gains = matmul(gains.astype(BF16), moved)[0:3]
    norms = jnp.concatenate(three_parts(norm_ref[...]), axis=0)
    zeros = jnp.zeros((3, 128), F32)
    tail = [
        gains,
        jnp.where(first_core, norms, zeros),
        jnp.where(first_core, zeros, norms),
        jnp.zeros((7, 128), F32),
    ]
    side_ref[128:144] = jnp.concatenate(tail, axis=0).astype(BF16)
    low = (lane == across).astype(F32).astype(BF16)
    high = (lane == across + channels).astype(F32).astype(BF16)
    rim = matmul(values[rows - 16 :], low)[0:8] + matmul(values[rows - 16 :], high)[8:16]
    docs = docs_ref[...].astype(F32)
    last_doc = docs[:, rows - 1 :]
    trailing = (docs == last_doc).astype(F32)
    sums = matmul(jnp.broadcast_to(trailing, (8, rows)).astype(BF16), values)
    parts = [matmul(part.astype(BF16), low)[0:1] for part in three_parts(sums)]
    count = jnp.sum(trailing, axis=1, keepdims=True)

    lines = [jnp.broadcast_to(routes_ref[k : k + 1].astype(F32), square) for k in (0, 1)]
    columns = [line.T for line in lines]
    before = iota(square, 0) < iota(square, 1)

    def counted(mask):
        return jnp.sum(mask.astype(F32), axis=0, keepdims=True)

    first_rank = counted((columns[0] == lines[0]) & before)
    second_rank = counted(columns[0] == lines[1]) + counted((columns[1] == lines[1]) & before)
    first_slot = lines[0][0:1] * 16.0 + first_rank
    second_slot = lines[1][0:1] * 16.0 + second_rank
    slots_ref[...] = jnp.concatenate(
        [first_slot, second_slot, docs, jnp.zeros((5, rows), F32)], axis=0
    )
    share = [weights_ref[k : k + 1] for k in (0, 1)]
    line = iota((256, rows), 0)
    row = iota((8, 128), 0)
    at = iota((8, 128), 1)
    in_sums = (at < channels) & (at % 4 == 3)
    for k in range(3):
        rim = jnp.where(in_sums & (row == k), parts[k], rim)
    doc_high = jnp.floor(last_doc * (1.0 / 128.0))
    doc_low = last_doc - doc_high * 128.0
    for k, value in enumerate((count, doc_high, doc_low)):
        rim = jnp.where((row == 3) & (at == 3 + 4 * k), value, rim)
    place = iota((256, 128), 1)
    message = jnp.broadcast_to(rim[None], (32, 8, 128)).reshape(256, 128)
    for half in (0, 1):
        slot = (line // 8 * 16 + line % 8 + 8 * half).astype(F32)
        is_first = slot == first_slot
        is_second = slot == second_slot
        weight = jnp.sum(
            jnp.where(is_first, share[0], 0.0) + jnp.where(is_second, share[1], 0.0),
            axis=1,
            keepdims=True,
        )
        chosen_first = jnp.sum(is_first.astype(F32), axis=1, keepdims=True)
        for k, value in enumerate((*three_parts(weight), chosen_first)):
            message = jnp.where(place == 1 + 4 * k + 16 * half, value, message)
    message = message.reshape(32, 8, 128).astype(BF16)
    message_ref[:, 0] = message
    message_ref[:, 1] = message
    copy.wait()
    for k in range(8):
        here = pl.ds(pl.multiple_of(256 * k + 128 * core_ref[0], 128), 128)
        there = pl.ds(pl.multiple_of(256 * k + 128 - 128 * core_ref[0], 128), 128)
        mine_ref[64 * k : 64 * (k + 1)] = project_ref[:, here]
        side_ref[144 + 64 * k : 208 + 64 * k] = project_ref[:, there]


def packing(*refs):
    sources, pack_ref, packed = refs[:4], refs[4], refs[5]
    copies, start = [], 0
    for k, source in enumerate(sources):
        rows = source.shape[0]
        copies.append(
            pltpu.make_async_copy(source, pack_ref.at[start : start + rows], packed.at[k])
        )
        copies[-1].start()
        start += rows
    for copy in copies:
        copy.wait()


def pooling(
    index_ref,
    arrived_ref,
    side_ref,
    other_ref,
    mine_ref,
    slots_ref,
    out_ref,
):
    rows = channels = 128
    own = index_ref[0]
    docs = slots_ref[2:3]
    first_doc = docs[:, 0:1]
    sides = side_ref[0:144].astype(F32) + other_ref[0:144].astype(F32)
    values = sides[0:128].astype(BF16)
    gain = sides[128:129] + (sides[129:130] + sides[130:131])
    meta = arrived_ref[:, 0].astype(F32)[:, 3:4]
    their_count = meta[:, :, 3:4]
    their_doc = meta[:, :, 7:8] * 128.0 + meta[:, :, 11:12]
    block = iota((32, 1, 1), 0)
    joins = (block < own) & (their_doc == first_doc.reshape(1, 1, 1))
    behind = block == own - 1
    carry_length = jnp.sum(jnp.where(joins, their_count, 0.0), axis=0)
    source = iota((128, 128), 0)
    target = iota((128, 128), 1)
    carry = jnp.zeros((8, 128), F32)
    upper_rim = jnp.zeros((8, 128), F32)
    lower_rim = jnp.zeros((8, 128), F32)
    for side in (0, 1):
        arrived = arrived_ref[:, side].astype(F32)
        sums = jnp.sum(jnp.where(joins, arrived, 0.0), axis=0)
        total = jnp.sum(jnp.where(iota((8, 128), 0) < 3, sums, 0.0), axis=0, keepdims=True)
        here = target - 64 * side
        inside = (here >= 0) & (here < 64)
        low = (inside & (source == here)).astype(F32).astype(BF16)
        high = (inside & (source == here + 64)).astype(F32).astype(BF16)
        for part in three_parts(total):
            carry = carry + matmul(jnp.broadcast_to(part, (8, 128)).astype(BF16), low)
        their_rim = jnp.sum(jnp.where(behind, arrived, 0.0), axis=0).astype(BF16)
        upper_rim = upper_rim + matmul(their_rim, low)
        lower_rim = lower_rim + matmul(their_rim, high)
    carry = carry[0:1]
    rim = jnp.concatenate([upper_rim, lower_rim], axis=0).astype(BF16)
    rim_rows = jnp.sum(jnp.where(behind & joins, their_count, 0.0), axis=0)

    square = (rows, rows)
    line = jnp.broadcast_to(docs, square)
    column = line.T
    here = iota(square, 0)
    there = iota(square, 1)
    together = (line == column) & (there <= here)
    opens = column[:, 0:1] == first_doc
    length = jnp.sum(together.astype(F32), axis=1, keepdims=True) + jnp.where(
        opens, carry_length, 0.0
    )
    position = iota((rows, 16), 0)
    back_by = 16 - iota((rows, 16), 1)
    rim_open = jnp.broadcast_to(opens, (rows, 16)) & (back_by.astype(F32) <= rim_rows)
    scale = iota((rows, channels), 1) % 4
    total = matmul(together.astype(F32).astype(BF16), values) + jnp.where(opens, carry, 0.0)
    amount = jnp.broadcast_to(length, (rows, channels))
    for k, window in ((0, 2), (1, 8), (2, 16)):
        mask = (together & (there > here - window)).astype(F32).astype(BF16)
        rim_mask = (rim_open & (position + back_by < window)).astype(F32).astype(BF16)
        part = matmul(mask, values) + matmul(rim_mask, rim)
        total = jnp.where(scale == k, part, total)
        amount = jnp.where(scale == k, jnp.minimum(length, float(window)), amount)
    pooled = ((total / amount - sides[0:128]) * gain).astype(BF16)
    first_core = index_ref[1] == 0
    pooled_own = jnp.where(first_core, pooled[:, :64].astype(F32), pooled[:, 64:].astype(F32))
    pooled_other = jnp.where(first_core, pooled[:, 64:].astype(F32), pooled[:, :64].astype(F32))
    pooled_own, pooled_other = pooled_own.astype(BF16), pooled_other.astype(BF16)
    tail = jnp.concatenate([sides[131:137], jnp.zeros((2, 128), F32)], axis=0).astype(BF16)
    for k in range(8):
        both = matmul(pooled_own, mine_ref[64 * k : 64 * (k + 1)])
        both = both + matmul(pooled_other, other_ref[144 + 64 * k : 208 + 64 * k])
        out_ref[k, 0:128] = both.astype(BF16)
        out_ref[k, 128:136] = tail


def sending(arrived_ref, slots_ref, residual_ref, hidden_ref, out_ref, gain_ref):
    projected = jnp.zeros((128, 128), F32)
    for k in range(8):
        projected = projected + arrived_ref[k, 0:128].astype(F32)
        tail = arrived_ref[k, 128:136].astype(F32)
        for side in (0, 1):
            part = tail[3 * side : 3 * side + 3]
            gain_ref[2 * k + side : 2 * k + side + 1] = part[0:1] + part[1:2] + part[2:3]
    hidden = residual_ref[...].astype(F32) + projected.astype(BF16).astype(F32)
    hidden_ref[...] = hidden
    slot = iota((512, 128), 0).astype(F32)
    chosen = (slot == slots_ref[0:1]) | (slot == slots_ref[1:2])
    picked = matmul(chosen.astype(F32).astype(BF16), hidden.astype(BF16))
    out_ref[...] = picked.reshape(64, 8, 128).astype(BF16)


def spreading(arrived_ref, out_ref):
    for k in range(8):
        out_ref[k] = arrived_ref[:, k % 2]


def experts(place_ref, x_ref, message_ref, gain_ref, *refs):
    sources, out_ref, normed_ref, sum_ref = refs[:12], refs[12], refs[13], refs[14]
    near, landed = refs[15:27], refs[27]
    gates, ups, lowers = near[0:4], near[4:8], near[8:12]
    copies = [
        pltpu.make_async_copy(sources[k], near[k], landed.at[k]) for k in range(12)
    ]
    for k in (0, 4, 1, 5, 2, 6, 8, 9, 10, 11, 3, 7):
        copies[k].start()

    squares = jnp.zeros((128, 128), F32)
    for k in range(16):
        part = x_ref[k // 2, :, k % 2].astype(F32).reshape(128, 128)
        squares = squares + part * part
    scaling = lax.rsqrt(jnp.sum(squares, axis=1, keepdims=True) * (1.0 / 2048.0) + 1e-06)
    for k in range(16):
        part = x_ref[k // 2, :, k % 2].astype(F32).reshape(128, 128)
        normed_ref[:, 128 * k : 128 * (k + 1)] = (part * scaling * gain_ref[k : k + 1]).astype(
            BF16
        )
    message = message_ref[:, 0].astype(F32).reshape(16, 2, 8, 128)
    side = jnp.where(place_ref[1] == 0, message[:, 0], message[:, 1]).reshape(128, 128)
    left = place_ref[0] == 0
    told = [jnp.where(left, side[:, k : k + 1], side[:, k + 16 : k + 17]) for k in (1, 5, 9, 13)]
    weight = told[0] + (told[1] + told[2])
    first = told[3]
    normed = normed_ref[...]

    def hidden(k):
        copies[k].wait()
        copies[k + 4].wait()
        lower = matmul(normed, gates[k][...])
        upper = matmul(normed, ups[k][...])
        return (jax.nn.silu(lower) * upper * weight).astype(BF16)

    early = [hidden(k) for k in range(3)]
    for copy in copies[8:]:
        copy.wait()
    across = jnp.concatenate(
        [pack[256:320] for pack in lowers] + [pack[320:384] for pack in lowers], axis=0
    )
    both = lax.dot_general(
        normed, across, (((1,), (1,)), ((), ())), preferred_element_type=F32
    )
    shared = (jax.nn.silu(both[:, :256]) * both[:, 256:] * first).astype(BF16)
    shared_down = jnp.concatenate([pack[384:448] for pack in lowers], axis=0)
    for k in range(8):
        cut = slice(256 * k, 256 * (k + 1))
        total = matmul(shared, shared_down[:, cut])
        for value, pack in zip(early, lowers):
            total = total + matmul(value, pack[0:256, cut])
        sum_ref[k] = total
    last = hidden(3)
    for k in range(8):
        cut = slice(256 * k, 256 * (k + 1))
        total = sum_ref[k] + matmul(last, lowers[3][0:256, cut])
        out_ref[k, :, 0] = total[:, :128].reshape(16, 8, 128).astype(BF16)
        out_ref[k, :, 1] = total[:, 128:].reshape(16, 8, 128).astype(BF16)


def adding(arrived_ref, out_ref):
    for side in (0, 1):
        total = arrived_ref[side].astype(F32)
        for k in range(2 + side, 8, 2):
            total = total + arrived_ref[k].astype(F32)
        out_ref[:, side] = total.astype(BF16)


def closing(arrived_ref, slots_ref, hidden_ref, out_ref):
    slot = iota((128, 512), 1).astype(F32)
    first = jnp.broadcast_to(slots_ref[0:1], (128, 128)).T[:, 0:1]
    second = jnp.broadcast_to(slots_ref[1:2], (128, 128)).T[:, 0:1]
    chosen = (slot == first) | (slot == second)
    arrived = arrived_ref[...].astype(F32).reshape(512, 128).astype(BF16)
    routed = matmul(chosen.astype(F32).astype(BF16), arrived)
    out_ref[...] = (hidden_ref[...] + routed).astype(BF16)


VMEM = pl.BlockSpec(memory_space=pltpu.VMEM)
SMEM = pl.BlockSpec(memory_space=pltpu.SMEM)


HBM = pl.BlockSpec(memory_space=pl.ANY)


def is_array(value):
    return not isinstance(value, tuple)


def spec_of(value):
    far = getattr(value, "memory_space", None) == pltpu.HBM
    return HBM if far else VMEM


def kernel(body, outs, operands, near=(), far=(), scalars=0, scratch=(), room=16):
    near = [pltpu.with_memory_space_constraint(value, pltpu.VMEM) for value in near]
    far = [pltpu.with_memory_space_constraint(value, pltpu.HBM) for value in far]
    scalar = operands[:scalars]
    plain = [
        pltpu.with_memory_space_constraint(value, pltpu.HBM) for value in operands[scalars:]
    ]
    return pl.pallas_call(
        body,
        out_shape=outs,
        in_specs=[SMEM] * scalars
        + [VMEM] * (len(near) + len(plain))
        + [HBM] * len(far),
        out_specs=jax.tree.map(spec_of, outs, is_leaf=is_array),
        scratch_shapes=scratch,
        compiler_params=pltpu.CompilerParams(vmem_limit_bytes=room * 2**20),
    )(*scalar, *near, *plain, *far)


def array(shape, kind):
    return pltpu.VMEM(shape, kind)


def body(
    pool_input,
    doc_ids,
    residual,
    pool_gain,
    out_proj,
    norm_gain,
    routes,
    route_weights,
    expert_gate,
    expert_up,
    expert_down,
    shared_gate,
    shared_up,
    shared_down,
):
    docs = doc_ids.reshape(1, 128)
    core = lax.axis_index("c").astype(jnp.int32)
    index = jnp.stack([lax.axis_index("sp").astype(jnp.int32), core])
    message, slots, side, mine = kernel(
        opening,
        (
            array((32, 2, 8, 128), BF16),
            array((8, 128), F32),
            array((656, 128), BF16),
            array((512, 128), BF16),
        ),
        (
            core.reshape(1),
            pool_input.T,
            docs,
            routes.T,
            route_weights.T,
            pool_gain.reshape(1, 64),
            norm_gain.reshape(1, 128),
        ),
        far=(out_proj,),
        scalars=1,
        scratch=[pltpu.VMEM((64, 2048), BF16), pltpu.SemaphoreType.DMA((1,))],
    )
    packed = kernel(
        packing,
        array((448, 2048), BF16),
        (),
        far=(expert_down[0], shared_gate.T, shared_up.T, shared_down),
        scratch=[pltpu.SemaphoreType.DMA((4,))],
    )
    groups = []
    for value in (expert_gate[0], expert_up[0], packed):
        ring = lax.ppermute(value, ("y", "c"), AROUND)
        own_other = lax.ppermute(value, "c", SWAP)
        ring_other = lax.ppermute(ring, "c", SWAP)
        groups += [value, own_other, ring, ring_other]
    arrived = exchanged(message.reshape(64, 8, 128), ("sp", "c"))
    arrived = arrived.reshape(32, 2, 8, 128)
    other_side = lax.ppermute(side, "c", SWAP)
    terms = kernel(
        pooling,
        array((8, 136, 128), BF16),
        (index,),
        near=(arrived, side, other_side, mine, slots),
        scalars=1,
    )
    terms = exchanged(terms, "y")
    hidden_state, outgoing, gains = kernel(
        sending,
        (array((128, 128), F32), array((64, 8, 128), BF16), array((16, 128), F32)),
        (),
        near=(terms, slots, residual),
    )
    rows = exchanged(outgoing, ("sp", "c"))
    rows = kernel(
        spreading, array((8, 16, 2, 8, 128), BF16), (), near=(rows.reshape(16, 2, 2, 8, 128),)
    )
    rows = exchanged(rows, "y")
    place = jnp.stack([core, lax.axis_index("y").astype(jnp.int32) & 1])
    parts = kernel(
        experts,
        array((8, 16, 2, 8, 128), BF16),
        (place,),
        near=(rows, arrived, gains),
        far=groups,
        scalars=1,
        scratch=[pltpu.VMEM((128, 2048), BF16), pltpu.VMEM((8, 128, 256), F32)]
        + [pltpu.VMEM(value.shape, BF16) for value in groups]
        + [pltpu.SemaphoreType.DMA((12,))],
        room=24,
    )
    parts = exchanged(parts, "y")
    summed = kernel(adding, array((16, 2, 2, 8, 128), BF16), (), near=(parts,))
    returned = exchanged(summed.reshape(64, 8, 128), ("sp", "c"))
    return kernel(
        closing, jax.ShapeDtypeStruct((128, 128), BF16), (), near=(returned, slots, hidden_state)
    )


def solution(mesh):
    split = Mesh(mesh.devices.reshape(32, 8, 2), ("sp", "y", "c"))
    tp = ("y", "c")
    placed = (
        P("sp", tp),
        P("sp"),
        P("sp", tp),
        P(tp),
        P(tp, None),
        P(tp),
        P("sp", None),
        P("sp", None),
        P("sp", None, tp),
        P("sp", None, tp),
        P("sp", tp, None),
        P(None, tp),
        P(None, tp),
        P(tp, None),
    )
    return jax.shard_map(body, mesh=split, in_specs=placed, out_specs=P("sp", tp), check_vma=False)
```

```python
import jax
import jax.numpy as jnp
from jax import lax
from jax.experimental import pallas as pl
from jax.experimental.pallas import tpu as pltpu
from jax.sharding import Mesh
from jax.sharding import PartitionSpec as P


F32 = jnp.float32
BF16 = jnp.bfloat16


SWAP = ((0, 1), (1, 0))
AROUND = tuple(
    (2 * y + c, 2 * ((y + (1 if c else -1)) % 8) + c) for y in range(8) for c in range(2)
)


def exchanged(value, axis):
    return lax.all_to_all(value, axis, split_axis=0, concat_axis=0, tiled=True)


def three_parts(value):
    first = value.astype(BF16).astype(F32)
    second = (value - first).astype(BF16).astype(F32)
    third = (value - first - second).astype(BF16).astype(F32)
    return first, second, third


def iota(shape, dim):
    return lax.broadcasted_iota(jnp.int32, shape, dim)


def matmul(a, b):
    return jnp.dot(a, b, preferred_element_type=F32)


def opening(
    core_ref,
    pool_ref,
    docs_ref,
    routes_ref,
    weights_ref,
    gain_ref,
    norm_ref,
    source_ref,
    message_ref,
    slots_ref,
    side_ref,
    mine_ref,
    project_ref,
    landed,
):
    copy = pltpu.make_async_copy(source_ref, project_ref, landed.at[0])
    copy.start()
    channels, rows = pool_ref.shape
    square = (rows, rows)
    values = pool_ref[...].astype(F32).T.astype(BF16)
    across = iota((channels, 128), 0)
    lane = iota((channels, 128), 1)
    first_core = core_ref[0] == 0
    moved = (lane == across + jnp.where(first_core, 0, channels)).astype(F32).astype(BF16)
    side_ref[0:128] = matmul(values, moved).astype(BF16)
    gains = jnp.concatenate([*three_parts(gain_ref[...]), jnp.zeros((5, channels), F32)], axis=0)
    gains = matmul(gains.astype(BF16), moved)[0:3]
    norms = jnp.concatenate(three_parts(norm_ref[...]), axis=0)
    zeros = jnp.zeros((3, 128), F32)
    tail = [
        gains,
        jnp.where(first_core, norms, zeros),
        jnp.where(first_core, zeros, norms),
        jnp.zeros((7, 128), F32),
    ]
    side_ref[128:144] = jnp.concatenate(tail, axis=0).astype(BF16)
    low = (lane == across).astype(F32).astype(BF16)
    high = (lane == across + channels).astype(F32).astype(BF16)
    rim = matmul(values[rows - 16 :], low)[0:8] + matmul(values[rows - 16 :], high)[8:16]
    docs = docs_ref[...].astype(F32)
    last_doc = docs[:, rows - 1 :]
    trailing = (docs == last_doc).astype(F32)
    sums = matmul(jnp.broadcast_to(trailing, (8, rows)).astype(BF16), values)
    parts = [matmul(part.astype(BF16), low)[0:1] for part in three_parts(sums)]
    count = jnp.sum(trailing, axis=1, keepdims=True)

    lines = [jnp.broadcast_to(routes_ref[k : k + 1].astype(F32), square) for k in (0, 1)]
    columns = [line.T for line in lines]
    before = iota(square, 0) < iota(square, 1)

    def counted(mask):
        return jnp.sum(mask.astype(F32), axis=0, keepdims=True)

    first_rank = counted((columns[0] == lines[0]) & before)
    second_rank = counted(columns[0] == lines[1]) + counted((columns[1] == lines[1]) & before)
    first_slot = lines[0][0:1] * 16.0 + first_rank
    second_slot = lines[1][0:1] * 16.0 + second_rank
    slots_ref[...] = jnp.concatenate(
        [first_slot, second_slot, docs, jnp.zeros((5, rows), F32)], axis=0
    )
    share = [weights_ref[k : k + 1] for k in (0, 1)]
    line = iota((256, rows), 0)
    row = iota((8, 128), 0)
    at = iota((8, 128), 1)
    in_sums = (at < channels) & (at % 4 == 3)
    for k in range(3):
        rim = jnp.where(in_sums & (row == k), parts[k], rim)
    doc_high = jnp.floor(last_doc * (1.0 / 128.0))
    doc_low = last_doc - doc_high * 128.0
    for k, value in enumerate((count, doc_high, doc_low)):
        rim = jnp.where((row == 3) & (at == 3 + 4 * k), value, rim)
    place = iota((256, 128), 1)
    message = jnp.broadcast_to(rim[None], (32, 8, 128)).reshape(256, 128)
    for half in (0, 1):
        slot = (line // 8 * 16 + line % 8 + 8 * half).astype(F32)
        is_first = slot == first_slot
        is_second = slot == second_slot
        weight = jnp.sum(
            jnp.where(is_first, share[0], 0.0) + jnp.where(is_second, share[1], 0.0),
            axis=1,
            keepdims=True,
        )
        chosen_first = jnp.sum(is_first.astype(F32), axis=1, keepdims=True)
        for k, value in enumerate((*three_parts(weight), chosen_first)):
            message = jnp.where(place == 1 + 4 * k + 16 * half, value, message)
    message = message.reshape(32, 8, 128).astype(BF16)
    message_ref[:, 0] = message
    message_ref[:, 1] = message
    copy.wait()
    for k in range(8):
        here = pl.ds(pl.multiple_of(256 * k + 128 * core_ref[0], 128), 128)
        there = pl.ds(pl.multiple_of(256 * k + 128 - 128 * core_ref[0], 128), 128)
        mine_ref[64 * k : 64 * (k + 1)] = project_ref[:, here]
        side_ref[144 + 64 * k : 208 + 64 * k] = project_ref[:, there]


def packing(*refs):
    sources, pack_ref, packed = refs[:4], refs[4], refs[5]
    copies, start = [], 0
    for k, source in enumerate(sources):
        rows = source.shape[0]
        copies.append(
            pltpu.make_async_copy(source, pack_ref.at[start : start + rows], packed.at[k])
        )
        copies[-1].start()
        start += rows
    for copy in copies:
        copy.wait()


def pooling(
    index_ref,
    arrived_ref,
    side_ref,
    other_ref,
    mine_ref,
    slots_ref,
    out_ref,
):
    rows = channels = 128
    own = index_ref[0]
    docs = slots_ref[2:3]
    first_doc = docs[:, 0:1]
    sides = side_ref[0:144].astype(F32) + other_ref[0:144].astype(F32)
    values = sides[0:128].astype(BF16)
    gain = sides[128:129] + (sides[129:130] + sides[130:131])
    meta = arrived_ref[:, 0].astype(F32)[:, 3:4]
    their_count = meta[:, :, 3:4]
    their_doc = meta[:, :, 7:8] * 128.0 + meta[:, :, 11:12]
    block = iota((32, 1, 1), 0)
    joins = (block < own) & (their_doc == first_doc.reshape(1, 1, 1))
    behind = block == own - 1
    carry_length = jnp.sum(jnp.where(joins, their_count, 0.0), axis=0)
    source = iota((128, 128), 0)
    target = iota((128, 128), 1)
    carry = jnp.zeros((8, 128), F32)
    upper_rim = jnp.zeros((8, 128), F32)
    lower_rim = jnp.zeros((8, 128), F32)
    for side in (0, 1):
        arrived = arrived_ref[:, side].astype(F32)
        sums = jnp.sum(jnp.where(joins, arrived, 0.0), axis=0)
        total = jnp.sum(jnp.where(iota((8, 128), 0) < 3, sums, 0.0), axis=0, keepdims=True)
        here = target - 64 * side
        inside = (here >= 0) & (here < 64)
        low = (inside & (source == here)).astype(F32).astype(BF16)
        high = (inside & (source == here + 64)).astype(F32).astype(BF16)
        for part in three_parts(total):
            carry = carry + matmul(jnp.broadcast_to(part, (8, 128)).astype(BF16), low)
        their_rim = jnp.sum(jnp.where(behind, arrived, 0.0), axis=0).astype(BF16)
        upper_rim = upper_rim + matmul(their_rim, low)
        lower_rim = lower_rim + matmul(their_rim, high)
    carry = carry[0:1]
    rim = jnp.concatenate([upper_rim, lower_rim], axis=0).astype(BF16)
    rim_rows = jnp.sum(jnp.where(behind & joins, their_count, 0.0), axis=0)

    square = (rows, rows)
    line = jnp.broadcast_to(docs, square)
    column = line.T
    here = iota(square, 0)
    there = iota(square, 1)
    together = (line == column) & (there <= here)
    opens = column[:, 0:1] == first_doc
    length = jnp.sum(together.astype(F32), axis=1, keepdims=True) + jnp.where(
        opens, carry_length, 0.0
    )
    position = iota((rows, 16), 0)
    back_by = 16 - iota((rows, 16), 1)
    rim_open = jnp.broadcast_to(opens, (rows, 16)) & (back_by.astype(F32) <= rim_rows)
    scale = iota((rows, channels), 1) % 4
    total = matmul(together.astype(F32).astype(BF16), values) + jnp.where(opens, carry, 0.0)
    amount = jnp.broadcast_to(length, (rows, channels))
    for k, window in ((0, 2), (1, 8), (2, 16)):
        mask = (together & (there > here - window)).astype(F32).astype(BF16)
        rim_mask = (rim_open & (position + back_by < window)).astype(F32).astype(BF16)
        part = matmul(mask, values) + matmul(rim_mask, rim)
        total = jnp.where(scale == k, part, total)
        amount = jnp.where(scale == k, jnp.minimum(length, float(window)), amount)
    pooled = ((total / amount - sides[0:128]) * gain).astype(BF16)
    first_core = index_ref[1] == 0
    pooled_own = jnp.where(first_core, pooled[:, :64].astype(F32), pooled[:, 64:].astype(F32))
    pooled_other = jnp.where(first_core, pooled[:, 64:].astype(F32), pooled[:, :64].astype(F32))
    pooled_own, pooled_other = pooled_own.astype(BF16), pooled_other.astype(BF16)
    tail = jnp.concatenate([sides[131:137], jnp.zeros((2, 128), F32)], axis=0).astype(BF16)
    for k in range(8):
        both = matmul(pooled_own, mine_ref[64 * k : 64 * (k + 1)])
        both = both + matmul(pooled_other, other_ref[144 + 64 * k : 208 + 64 * k])
        out_ref[k, 0:128] = both.astype(BF16)
        out_ref[k, 128:136] = tail


def sending(arrived_ref, slots_ref, residual_ref, hidden_ref, out_ref, gain_ref):
    projected = jnp.zeros((128, 128), F32)
    for k in range(8):
        projected = projected + arrived_ref[k, 0:128].astype(F32)
        tail = arrived_ref[k, 128:136].astype(F32)
        for side in (0, 1):
            part = tail[3 * side : 3 * side + 3]
            gain_ref[2 * k + side : 2 * k + side + 1] = part[0:1] + part[1:2] + part[2:3]
    hidden = residual_ref[...].astype(F32) + projected.astype(BF16).astype(F32)
    hidden_ref[...] = hidden
    slot = iota((512, 128), 0).astype(F32)
    chosen = (slot == slots_ref[0:1]) | (slot == slots_ref[1:2])
    picked = matmul(chosen.astype(F32).astype(BF16), hidden.astype(BF16))
    out_ref[...] = picked.reshape(64, 8, 128).astype(BF16)


def spreading(arrived_ref, out_ref):
    for k in range(8):
        out_ref[k] = arrived_ref[:, k % 2]


def experts(place_ref, x_ref, message_ref, gain_ref, gate_ref, *refs):
    sources, out_ref, normed_ref, sum_ref = refs[:11], refs[11], refs[12], refs[13]
    near, landed = refs[14:25], refs[25]
    gates, ups, lowers = (gate_ref, *near[0:3]), near[3:7], near[7:11]
    copies = [
        pltpu.make_async_copy(sources[k], near[k], landed.at[k]) for k in range(11)
    ]
    for k in (3, 0, 4, 1, 5, 7, 8, 9, 10, 2, 6):
        copies[k].start()

    squares = jnp.zeros((128, 128), F32)
    for k in range(16):
        part = x_ref[k // 2, :, k % 2].astype(F32).reshape(128, 128)
        squares = squares + part * part
    scaling = lax.rsqrt(jnp.sum(squares, axis=1, keepdims=True) * (1.0 / 2048.0) + 1e-06)
    for k in range(16):
        part = x_ref[k // 2, :, k % 2].astype(F32).reshape(128, 128)
        normed_ref[:, 128 * k : 128 * (k + 1)] = (part * scaling * gain_ref[k : k + 1]).astype(
            BF16
        )
    message = message_ref[:, 0].astype(F32).reshape(16, 2, 8, 128)
    side = jnp.where(place_ref[1] == 0, message[:, 0], message[:, 1]).reshape(128, 128)
    left = place_ref[0] == 0
    told = [jnp.where(left, side[:, k : k + 1], side[:, k + 16 : k + 17]) for k in (1, 5, 9, 13)]
    weight = told[0] + (told[1] + told[2])
    first = told[3]
    normed = normed_ref[...]

    def hidden(k):
        if k > 0:
            copies[k - 1].wait()
        copies[k + 3].wait()
        lower = matmul(normed, gates[k][...])
        upper = matmul(normed, ups[k][...])
        return (jax.nn.silu(lower) * upper * weight).astype(BF16)

    early = [hidden(k) for k in range(3)]
    for copy in copies[7:]:
        copy.wait()
    across = jnp.concatenate(
        [pack[256:320] for pack in lowers] + [pack[320:384] for pack in lowers], axis=0
    )
    both = lax.dot_general(
        normed, across, (((1,), (1,)), ((), ())), preferred_element_type=F32
    )
    shared = (jax.nn.silu(both[:, :256]) * both[:, 256:] * first).astype(BF16)
    shared_down = jnp.concatenate([pack[384:448] for pack in lowers], axis=0)
    for k in range(8):
        cut = slice(256 * k, 256 * (k + 1))
        total = matmul(shared, shared_down[:, cut])
        for value, pack in zip(early, lowers):
            total = total + matmul(value, pack[0:256, cut])
        sum_ref[k] = total
    last = hidden(3)
    for k in range(8):
        cut = slice(256 * k, 256 * (k + 1))
        total = sum_ref[k] + matmul(last, lowers[3][0:256, cut])
        out_ref[k, :, 0] = total[:, :128].reshape(16, 8, 128).astype(BF16)
        out_ref[k, :, 1] = total[:, 128:].reshape(16, 8, 128).astype(BF16)


def adding(arrived_ref, out_ref):
    for side in (0, 1):
        total = arrived_ref[side].astype(F32)
        for k in range(2 + side, 8, 2):
            total = total + arrived_ref[k].astype(F32)
        out_ref[:, side] = total.astype(BF16)


def closing(arrived_ref, slots_ref, hidden_ref, out_ref):
    slot = iota((128, 512), 1).astype(F32)
    first = jnp.broadcast_to(slots_ref[0:1], (128, 128)).T[:, 0:1]
    second = jnp.broadcast_to(slots_ref[1:2], (128, 128)).T[:, 0:1]
    chosen = (slot == first) | (slot == second)
    arrived = arrived_ref[...].astype(F32).reshape(512, 128).astype(BF16)
    routed = matmul(chosen.astype(F32).astype(BF16), arrived)
    out_ref[...] = (hidden_ref[...] + routed).astype(BF16)


VMEM = pl.BlockSpec(memory_space=pltpu.VMEM)
SMEM = pl.BlockSpec(memory_space=pltpu.SMEM)


HBM = pl.BlockSpec(memory_space=pl.ANY)


def is_array(value):
    return not isinstance(value, tuple)


def spec_of(value):
    far = getattr(value, "memory_space", None) == pltpu.HBM
    return HBM if far else VMEM


def kernel(body, outs, operands, near=(), far=(), scalars=0, scratch=(), room=16):
    near = [pltpu.with_memory_space_constraint(value, pltpu.VMEM) for value in near]
    far = [pltpu.with_memory_space_constraint(value, pltpu.HBM) for value in far]
    scalar = operands[:scalars]
    plain = [
        pltpu.with_memory_space_constraint(value, pltpu.HBM) for value in operands[scalars:]
    ]
    return pl.pallas_call(
        body,
        out_shape=outs,
        in_specs=[SMEM] * scalars
        + [VMEM] * (len(near) + len(plain))
        + [HBM] * len(far),
        out_specs=jax.tree.map(spec_of, outs, is_leaf=is_array),
        scratch_shapes=scratch,
        compiler_params=pltpu.CompilerParams(vmem_limit_bytes=room * 2**20),
    )(*scalar, *near, *plain, *far)


def array(shape, kind):
    return pltpu.VMEM(shape, kind)


def body(
    pool_input,
    doc_ids,
    residual,
    pool_gain,
    out_proj,
    norm_gain,
    routes,
    route_weights,
    expert_gate,
    expert_up,
    expert_down,
    shared_gate,
    shared_up,
    shared_down,
):
    docs = doc_ids.reshape(1, 128)
    core = lax.axis_index("c").astype(jnp.int32)
    index = jnp.stack([lax.axis_index("sp").astype(jnp.int32), core])
    message, slots, side, mine = kernel(
        opening,
        (
            array((32, 2, 8, 128), BF16),
            array((8, 128), F32),
            array((656, 128), BF16),
            array((512, 128), BF16),
        ),
        (
            core.reshape(1),
            pool_input.T,
            docs,
            routes.T,
            route_weights.T,
            pool_gain.reshape(1, 64),
            norm_gain.reshape(1, 128),
        ),
        far=(out_proj,),
        scalars=1,
        scratch=[pltpu.VMEM((64, 2048), BF16), pltpu.SemaphoreType.DMA((1,))],
    )
    packed = kernel(
        packing,
        array((448, 2048), BF16),
        (),
        far=(expert_down[0], shared_gate.T, shared_up.T, shared_down),
        scratch=[pltpu.SemaphoreType.DMA((4,))],
    )
    groups = []
    for value in (expert_gate[0], expert_up[0], packed):
        ring = lax.ppermute(value, ("y", "c"), AROUND)
        own_other = lax.ppermute(value, "c", SWAP)
        ring_other = lax.ppermute(ring, "c", SWAP)
        groups += [value, own_other, ring, ring_other]
    arrived = exchanged(message.reshape(64, 8, 128), ("sp", "c"))
    arrived = arrived.reshape(32, 2, 8, 128)
    other_side = lax.ppermute(side, "c", SWAP)
    terms = kernel(
        pooling,
        array((8, 136, 128), BF16),
        (index,),
        near=(arrived, side, other_side, mine, slots),
        scalars=1,
    )
    terms = exchanged(terms, "y")
    hidden_state, outgoing, gains = kernel(
        sending,
        (array((128, 128), F32), array((64, 8, 128), BF16), array((16, 128), F32)),
        (),
        near=(terms, slots, residual),
    )
    rows = exchanged(outgoing, ("sp", "c"))
    rows = kernel(
        spreading, array((8, 16, 2, 8, 128), BF16), (), near=(rows.reshape(16, 2, 2, 8, 128),)
    )
    rows = exchanged(rows, "y")
    place = jnp.stack([core, lax.axis_index("y").astype(jnp.int32) & 1])
    parts = kernel(
        experts,
        array((8, 16, 2, 8, 128), BF16),
        (place,),
        near=(rows, arrived, gains, groups[0]),
        far=groups[1:],
        scalars=1,
        scratch=[pltpu.VMEM((128, 2048), BF16), pltpu.VMEM((8, 128, 256), F32)]
        + [pltpu.VMEM(value.shape, BF16) for value in groups[1:]]
        + [pltpu.SemaphoreType.DMA((11,))],
        room=24,
    )
    parts = exchanged(parts, "y")
    summed = kernel(adding, array((16, 2, 2, 8, 128), BF16), (), near=(parts,))
    returned = exchanged(summed.reshape(64, 8, 128), ("sp", "c"))
    return kernel(
        closing, jax.ShapeDtypeStruct((128, 128), BF16), (), near=(returned, slots, hidden_state)
    )


def solution(mesh):
    split = Mesh(mesh.devices.reshape(32, 8, 2), ("sp", "y", "c"))
    tp = ("y", "c")
    placed = (
        P("sp", tp),
        P("sp"),
        P("sp", tp),
        P(tp),
        P(tp, None),
        P(tp),
        P("sp", None),
        P("sp", None),
        P("sp", None, tp),
        P("sp", None, tp),
        P("sp", tp, None),
        P(None, tp),
        P(None, tp),
        P(tp, None),
    )
    return jax.shard_map(body, mesh=split, in_specs=placed, out_specs=P("sp", tp), check_vma=False)
```
